768 devices in a mesh: ep: 48 (over z, x), tp: 16 (over y, core).
Axes of the slice: x: 4, y: 8, z: 12, core: 2. Of those that a mesh axis runs over, the one named last changes fastest.
Arguments:
- tokens: bfloat16 [768, 2048], P('ep'), may hold values from -6 to 6
- attn_gain: bfloat16 [2048], replicated, may hold values from 0.099609375 to 1.8984375
- ffn_gain: bfloat16 [2048], replicated, may hold values from 0.099609375 to 1.8984375
- w_query: bfloat16 [2048, 2048], P(None, 'tp'), may hold values from -0.125 to 0.125
- w_key: bfloat16 [2048, 256], replicated, may hold values from -0.125 to 0.125
- w_value: bfloat16 [2048, 256], replicated, may hold values from -0.125 to 0.125
- w_forget: bfloat16 [2048, 32], replicated, may hold values from -0.125 to 0.125
- forget_bias: float32 [32], replicated, may hold values from -1 to 3
- w_out: bfloat16 [2048, 2048], P(None, 'tp'), may hold values from -0.375 to 0.375
- cache_keys: bfloat16 [768, 2048, 256], P(('ep', 'tp')), may hold values from -800 to 800
- cache_values: bfloat16 [768, 2048, 256], P(('ep', 'tp')), may hold values from -6 to 6
- cache_logcum: float32 [768, 32, 2048], P(('ep', 'tp')), as said below
- cache_len: int32 [768], P(('ep', 'tp')), may hold values from 256 to 2048
- route_group: int32 [768], P('ep'), may hold values from 0 to 3, as said below
- route_expert: int32 [768, 2], P('ep'), may hold values from 0 to 11, as said below
- route_weight: float32 [768, 2], P('ep'), may hold values from 0.2 to 1
- w_gate: bfloat16 [48, 2048, 2048], P('ep', None, 'tp'), may hold values from -0.125 to 0.125
- w_up: bfloat16 [48, 2048, 2048], P('ep', None, 'tp'), may hold values from -0.125 to 0.125
- w_down: bfloat16 [48, 2048, 2048], P('ep', None, 'tp'), may hold values from -0.125 to 0.125
Outputs:
- layer_out: bfloat16 [768, 2048], P('ep', 'tp')
The draws below stay inside these ranges and needn't reach their ends.
Inputs may be any that keep to these rules, and one draw needn't show every extreme that they name: Expert groups. Among the 16 sequences of one index of ep no expert route_group * 12 + route_expert is named more than 2 times, and in every draw one expert is named exactly 2 times by the sequences of every index of ep. `route_expert`: the 2 numbers of a sequence differ. `cache_logcum`: each entry is the sum of the log forget gates of that head from the first cached position up to and including that position.
All inputs are finite; a program needn't handle non-finite values.
Results may differ from the reference program's by a relative error of at most 0.012.
The reference program's roundings to bfloat16 on the way count: a program that leaves them out, or rounds other values in their place, can miss the bound.
Values may be sent and summed in bfloat16 or wider, within the bound.
A program may use at most 32 MiB of HBM per device.

```python
import math
import jax
import jax.numpy as jnp
from jax import lax

D = 2048
QUERY_HEAD_COUNT = 32
KV_HEADS = 4
HEAD = 64
FE = 2048
GROUPS = 4
TOP = 2
CACHE_LENGTH = 2048
GROUP_SEQS = 16
SEQUENCE_TOTAL = 768
EXPERTS = 48
CAP = 2
N_EP = 48


def draw_cache_keys(key, part):
    random_subkeys = jax.random.split(jax.random.fold_in(key, 3), 1)
    base_keys = jnp.clip(jax.random.normal(random_subkeys[0], (SEQUENCE_TOTAL, CACHE_LENGTH, KV_HEADS * HEAD), jnp.float32), -6.0, 6.0)
    return base_keys.astype(jnp.bfloat16)


def draw_cache_logcum(key, part):
    random_subkeys = jax.random.split(jax.random.fold_in(key, 5), 8)
    slow_heads = jax.random.bernoulli(random_subkeys[0], 0.5, (QUERY_HEAD_COUNT,))
    jitter = jnp.exp(jax.random.uniform(random_subkeys[6], (SEQUENCE_TOTAL, QUERY_HEAD_COUNT, CACHE_LENGTH), jnp.float32, math.log(0.3), math.log(3.0)))
    slow_rate = jnp.exp(jax.random.uniform(random_subkeys[1], (QUERY_HEAD_COUNT,), jnp.float32, math.log(0.2), math.log(0.6))) / CACHE_LENGTH
    fast_rate = 1.0 / jnp.exp(jax.random.uniform(random_subkeys[2], (QUERY_HEAD_COUNT,), jnp.float32, math.log(30.0), math.log(100.0)))
    decay_rate = jnp.where(slow_heads, slow_rate, fast_rate)
    seq_factor = jnp.exp(jax.random.uniform(random_subkeys[3], (SEQUENCE_TOTAL, 1, 1), jnp.float32, math.log(0.5), math.log(2.0)))
    block_factor = jnp.exp(jax.random.uniform(random_subkeys[4], (SEQUENCE_TOTAL, 1, 16), jnp.float32, math.log(0.7), math.log(1.4)))
    cache_position = jnp.arange(CACHE_LENGTH)
    block_index = cache_position * 16 // CACHE_LENGTH
    block_scale = block_factor[:, :, block_index]
    step_increments = -decay_rate[None, :, None] * seq_factor * block_scale * jitter
    spike_events = jax.random.randint(random_subkeys[5], (SEQUENCE_TOTAL, 3), 0, CACHE_LENGTH)
    spike_penalty = jnp.log(jax.random.uniform(random_subkeys[7], (SEQUENCE_TOTAL, 3), jnp.float32, 0.5, 0.8))
    match_counts = (cache_position[None, None, :] == spike_events[:, :, None]).astype(jnp.float32)
    step_increments = step_increments + jnp.sum(match_counts * spike_penalty[:, :, None], axis=1)[:, None, :]
    return jnp.cumsum(step_increments, axis=-1)


def routing_draw(key):
    random_subkeys = jax.random.split(key, 6)
    per_group = EXPERTS // GROUPS
    heavy_group = jax.random.randint(random_subkeys[0], (), 0, GROUPS)
    heavy_perm = jax.random.permutation(random_subkeys[1], per_group)
    fewest_rows = per_group * (CAP - 1) // TOP + 1
    heavy_rows = min(per_group * CAP // TOP, GROUP_SEQS)
    heavy_count = jax.random.randint(random_subkeys[2], (N_EP, 1), fewest_rows, heavy_rows + 1)
    row_order = jax.vmap(lambda subkey: jax.random.permutation(subkey, GROUP_SEQS))(jax.random.split(random_subkeys[3], N_EP))
    other_group = (heavy_group + 1 + jax.random.randint(random_subkeys[4], (N_EP, GROUP_SEQS), 0, GROUPS - 1)) % GROUPS
    group_ids = jnp.where(row_order < heavy_count, heavy_group, other_group)
    same_group = group_ids[:, :, None] == group_ids[:, None, :]
    earlier = row_order[:, None, :] < row_order[:, :, None]
    rank_in_group = jnp.sum((same_group & earlier).astype(jnp.int32), axis=2)
    group_perms = jax.vmap(lambda subkey: jax.random.permutation(subkey, per_group))(jax.random.split(random_subkeys[5], N_EP * GROUPS))
    group_perms = group_perms.reshape(N_EP, GROUPS, per_group)
    group_perms = jnp.where(jnp.arange(GROUPS)[None, :, None] == heavy_group, heavy_perm[None, None, :], group_perms)
    row_table = jnp.take_along_axis(group_perms, group_ids[:, :, None], axis=1)
    picks = []
    for choice_index in range(TOP):
        slot_index = (TOP * rank_in_group + choice_index) % per_group
        picks.append(jnp.take_along_axis(row_table, slot_index[:, :, None], axis=2)[:, :, 0])
    experts_local = jnp.stack(picks, axis=-1)
    return (group_ids.reshape(SEQUENCE_TOTAL).astype(jnp.int32), experts_local.reshape(SEQUENCE_TOTAL, TOP).astype(jnp.int32))


def draw_route_group(key, part):
    return routing_draw(jax.random.fold_in(key, 17))[0]


def draw_route_expert(key, part):
    return routing_draw(jax.random.fold_in(key, 17))[1]


def place_ends(values, key, low, largest):
    longest = values.shape.index(max(values.shape))
    spots = []
    for shift in (0, 1):
        where = [jax.random.randint(jax.random.fold_in(key, axis), (), 0, length) for axis, length in enumerate(values.shape)]
        where[longest] = (where[longest] + shift) % values.shape[longest]
        spots.append(tuple(where))
    return values.at[spots[0]].set(low).at[spots[1]].set(largest)


def level_of(rng, extent, cuts, least, largest):
    factor_of = 1.0
    for dim, blocks in cuts:
        steps = jax.random.uniform(jax.random.fold_in(jax.random.fold_in(rng, 6), dim), (blocks,), jnp.float32, least / len(cuts), largest / len(cuts))
        factor_of = factor_of * jnp.repeat(jnp.exp(steps), extent[dim] // blocks).reshape((-1,) + (1,) * (len(extent) - 1 - dim))
    return factor_of


def centred(key, shape, scale, limit, cuts=(), kind=jnp.bfloat16):
    drawn = scale * jax.random.normal(key, shape, jnp.float32)
    if cuts:
        drawn = drawn * level_of(key, shape, cuts, -0.22, 0.18)
    return jnp.clip(drawn, -limit, limit).astype(kind)


def setup_inputs(seed: int = 0) -> dict:
    streams_of = jax.random.split(jax.random.key(seed), 20)
    tokens = centred(streams_of[0], (SEQUENCE_TOTAL, D), 1.0, 6.0, ((0, 48),))
    attn_gain = jnp.clip(1.0 + 0.18 * jax.random.normal(streams_of[1], (D,), jnp.float32), 0.099609375, 1.8984375).astype(jnp.bfloat16)
    ffn_gain = jnp.clip(1.0 + 0.18 * jax.random.normal(streams_of[2], (D,), jnp.float32), 0.099609375, 1.8984375).astype(jnp.bfloat16)
    w_query = centred(streams_of[3], (D, QUERY_HEAD_COUNT * HEAD), D ** -0.5, 0.125, ((1, 16),))
    w_key = centred(streams_of[4], (D, KV_HEADS * HEAD), D ** -0.5, 0.125)
    w_value = centred(streams_of[5], (D, KV_HEADS * HEAD), D ** -0.5, 0.125)
    w_forget = centred(streams_of[6], (D, QUERY_HEAD_COUNT), D ** -0.5, 0.125)
    forget_bias = jnp.clip(jax.random.uniform(streams_of[7], (QUERY_HEAD_COUNT,), jnp.float32, -1.0, 3.0), -1.0, 3.0)
    w_out = centred(streams_of[8], (QUERY_HEAD_COUNT * HEAD, D), (QUERY_HEAD_COUNT * HEAD // 8) ** -0.5, 0.375, ((1, 16),))
    cache_keys = draw_cache_keys(jax.random.fold_in(streams_of[19], 71), 0)
    cache_values = centred(streams_of[10], (SEQUENCE_TOTAL, CACHE_LENGTH, KV_HEADS * HEAD), 1.0, 6.0, ((0, 768),))
    cache_logcum = draw_cache_logcum(jax.random.fold_in(streams_of[19], 71), 0)
    cache_len = place_ends(jax.random.randint(streams_of[12], (SEQUENCE_TOTAL,), CACHE_LENGTH // 8, CACHE_LENGTH + 1), jax.random.fold_in(streams_of[12], 1), CACHE_LENGTH // 8, CACHE_LENGTH).astype(jnp.int32)
    route_group = draw_route_group(jax.random.fold_in(streams_of[19], 71), 0)
    route_expert = draw_route_expert(jax.random.fold_in(streams_of[19], 71), 0)
    route_weight = jnp.clip(jnp.exp(math.log(1.0) - 1.609438 * jax.random.uniform(streams_of[15], (SEQUENCE_TOTAL, TOP), jnp.float32) ** level_of(streams_of[15], (SEQUENCE_TOTAL, TOP), ((0, 48),), -0.2, 0.2)), 0.2, 1.0)
    w_gate = centred(streams_of[16], (EXPERTS, D, FE), D ** -0.5, 0.125, ((0, 48), (2, 16)))
    w_up = centred(streams_of[17], (EXPERTS, D, FE), D ** -0.5, 0.125, ((0, 48), (2, 16)))
    w_down = centred(streams_of[18], (EXPERTS, FE, D), FE ** -0.5, 0.125, ((0, 48), (2, 16)))
    return dict(tokens=tokens, attn_gain=attn_gain, ffn_gain=ffn_gain, w_query=w_query, w_key=w_key, w_value=w_value, w_forget=w_forget, forget_bias=forget_bias, w_out=w_out, cache_keys=cache_keys, cache_values=cache_values, cache_logcum=cache_logcum, cache_len=cache_len, route_group=route_group, route_expert=route_expert, route_weight=route_weight, w_gate=w_gate, w_up=w_up, w_down=w_down)


NORM_EPSILON = 1e-06
MASKED_SCORE = -1e+30

def normalize(values, gain_vec):
    return values * lax.rsqrt(lax.optimization_barrier(jnp.mean(values * values, axis=-1, keepdims=True)) + NORM_EPSILON) * gain_vec.astype(jnp.float32)

def attend_block(arguments):
    query, key_new, value_new, log_gate, keys, cached_values, logcum, lengths = arguments
    count_of_rows = query.shape[0]
    length = keys.shape[1]
    per_kv = QUERY_HEAD_COUNT // KV_HEADS
    score_scale = HEAD ** (-0.5)
    query_float = query.astype(jnp.float32).reshape(count_of_rows, KV_HEADS, per_kv, HEAD)
    keys_f = keys.astype(jnp.float32).reshape(count_of_rows, length, KV_HEADS, HEAD)
    scores = jnp.einsum('bkgd,blkd->bkgl', query_float, keys_f).reshape(count_of_rows, QUERY_HEAD_COUNT, length) * score_scale
    latest = jnp.take_along_axis(logcum, (lengths - 1).astype(jnp.int32)[:, None, None], axis=2)
    scores = scores + latest + log_gate[:, :, None] - logcum
    usable = jnp.arange(length, dtype=jnp.int32)[None, None, :] < lengths[:, None, None]
    scores = jnp.where(usable, scores, MASKED_SCORE)
    current_key = key_new.astype(jnp.float32).reshape(count_of_rows, KV_HEADS, HEAD)
    current_score = jnp.einsum('cnpx,cnx->cnp', query_float, current_key).reshape(count_of_rows, QUERY_HEAD_COUNT) * score_scale
    peak = jnp.maximum(lax.optimization_barrier(jnp.max(scores, axis=2)), current_score)
    weights = jnp.where(usable, jnp.exp(scores - peak[:, :, None]), 0.0)
    own_weight = jnp.exp(current_score - peak)
    denominator = lax.optimization_barrier(jnp.sum(weights, axis=2)) + own_weight
    weights_b = lax.optimization_barrier(weights.astype(jnp.bfloat16)).astype(jnp.float32)
    own_b = lax.optimization_barrier(own_weight.astype(jnp.bfloat16)).astype(jnp.float32)
    values_f = cached_values.astype(jnp.float32).reshape(count_of_rows, length, KV_HEADS, HEAD)
    summed = jnp.einsum('bkgl,blkd->bkgd', weights_b.reshape(count_of_rows, KV_HEADS, per_kv, length), values_f)
    own_value = value_new.astype(jnp.float32).reshape(count_of_rows, KV_HEADS, 1, HEAD)
    summed = summed + own_b.reshape(count_of_rows, KV_HEADS, per_kv)[..., None] * own_value
    summed = summed.reshape(count_of_rows, QUERY_HEAD_COUNT, HEAD) / denominator[:, :, None]
    return summed.reshape(count_of_rows, QUERY_HEAD_COUNT * HEAD).astype(jnp.bfloat16)

def reference(tokens, attn_gain, ffn_gain, w_query, w_key, w_value, w_forget, forget_bias, w_out, cache_keys, cache_values, cache_logcum, cache_len, route_group, route_expert, route_weight, w_gate, w_up, w_down):
    stream = tokens.astype(jnp.float32)
    normed = normalize(stream, attn_gain).astype(jnp.bfloat16)
    query = jnp.dot(normed, w_query, preferred_element_type=jnp.float32).astype(jnp.bfloat16)
    key_new = jnp.dot(normed, w_key, preferred_element_type=jnp.float32).astype(jnp.bfloat16)
    value_new = jnp.dot(normed, w_value, preferred_element_type=jnp.float32).astype(jnp.bfloat16)
    log_gate = jax.nn.log_sigmoid(jnp.dot(normed, w_forget, preferred_element_type=jnp.float32) + forget_bias.astype(jnp.float32))

    def by_group(array):
        return array.reshape((N_EP, GROUP_SEQS) + array.shape[1:])
    pieces = tuple((by_group(array) for array in (query, key_new, value_new, log_gate, cache_keys, cache_values, cache_logcum, cache_len)))
    attended = lax.map(attend_block, pieces).reshape(SEQUENCE_TOTAL, QUERY_HEAD_COUNT * HEAD)
    mixed = (stream + jnp.dot(attended, w_out, preferred_element_type=jnp.float32)).astype(jnp.bfloat16)
    inputs = normalize(mixed.astype(jnp.float32), ffn_gain).astype(jnp.bfloat16)
    experts_per_group = EXPERTS // GROUPS
    picked_ids = (route_group[:, None] * experts_per_group + route_expert).reshape(-1).astype(jnp.int32)
    max_rows = N_EP * CAP
    pick_count = SEQUENCE_TOTAL * TOP

    def one_expert(collected, expert_item):
        gate_weight, up_weight, down_weight, expert_index = expert_item
        chosen = jnp.nonzero(picked_ids == expert_index, size=max_rows, fill_value=pick_count)[0]
        row_data = inputs[jnp.minimum(chosen, pick_count - 1) // TOP]
        gate_proj = jnp.dot(row_data, gate_weight, preferred_element_type=jnp.float32)
        up_proj = jnp.dot(row_data, up_weight, preferred_element_type=jnp.float32)
        hidden = (jax.nn.silu(gate_proj) * up_proj).astype(jnp.bfloat16)
        result = jnp.dot(hidden, down_weight, preferred_element_type=jnp.float32).astype(jnp.bfloat16)
        result = lax.optimization_barrier(result).astype(jnp.float32)
        return (collected.at[chosen].set(result, mode='drop'), None)
    expert_order = jnp.arange(EXPERTS, dtype=jnp.int32)
    picked, _ = lax.scan(one_expert, jnp.zeros((pick_count, D), jnp.float32), (w_gate, w_up, w_down, expert_order))
    moe_sum = lax.optimization_barrier(jnp.sum(route_weight.astype(jnp.float32)[:, :, None] * picked.reshape(SEQUENCE_TOTAL, TOP, D), axis=1))
    return (mixed.astype(jnp.float32) + moe_sum).astype(jnp.bfloat16)
```

```python
import functools

import jax
import jax.numpy as jnp
from jax import lax
from jax.experimental import pallas as pl
from jax.experimental.pallas import tpu as pltpu
from jax.sharding import PartitionSpec as P

HEADS = 32
KV_HEADS = 4
HEAD = 64
GROUPS = 4
EPSILON = 1e-06
MASKED_SCORE = -1e30
SLOTS = 2
BF = jnp.bfloat16
F32 = jnp.float32
MESH = pl.DeviceIdType.MESH


def iota(shape, dim):
    return lax.broadcasted_iota(jnp.int32, shape, dim)


def dot(a, b):
    return jnp.dot(a, b, preferred_element_type=F32)


def dot_t(a, b):
    return lax.dot_general(a, b, (((1,), (1,)), ((), ())), preferred_element_type=F32)


def exact_parts(x):
    a = x.astype(BF)
    r = x - a.astype(F32)
    b = r.astype(BF)
    return a, b, (r - b.astype(F32)).astype(BF)


def layer_kernel(n_ep, n_tp, *refs):
    inputs, out_ref, rest = refs[:19], refs[19], refs[20:]
    held, scratch = rest[:18], rest[18:]
    (tok, again, fgain, wq, wk, wv, wf, fb, wo, ck, cv, lc, rg, re, rw, wg, wu, wd) = held
    len_ref = scratch[-1]
    sources = inputs[:12] + inputs[13:]
    (
        q_send, q_recv, att_all, att_rows, d_send, d_recv, x_all, h_all, r_send, r_recv,
        in_sem, q_ss, q_rs, a_ss, a_rs, d_ss, d_rs, x_ss, x_rs, x_fs, x_ps, h_ss, h_rs, h_fs, h_ps,
        r_ss, r_rs, len_sem, _,
    ) = scratch
    e = lax.axis_index("ep")
    t = lax.axis_index("tp")
    n_y = n_tp // 2
    y, c = t // 2, t % 2
    rows = tok.shape[0]
    picks = n_ep * SLOTS
    width = wo.shape[1]

    def ep_peer(i):
        k = (i + 1) // 2
        return lax.rem(e + n_ep // 2 + k * (1 - 2 * (i % 2)) + n_ep, n_ep)

    def tp_peer(i):
        k = (i + 1) // 2
        return lax.rem(t + n_tp // 2 + k * (1 - 2 * (i % 2)) + n_tp, n_tp)

    def loads(i):
        return pltpu.make_async_copy(sources[i], held[i], in_sem.at[i])

    for i in (0, 1, 3, 4, 5, 6, 7, 9, 11, 10, 12, 13, 14, 8, 2, 15, 16, 17):
        loads(i).start()
    load_len = pltpu.make_async_copy(inputs[12], len_ref, len_sem)
    load_len.start()

    barrier = pltpu.get_barrier_semaphore()

    @pl.loop(0, n_tp - 1)
    def _(i):
        pl.semaphore_signal(barrier, inc=1, device_id=(e, tp_peer(i)), device_id_type=MESH)

    @pl.loop(0, n_ep - 1)
    def _(i):
        pl.semaphore_signal(barrier, inc=1, device_id=(ep_peer(i), t), device_id_type=MESH)

    loads(0).wait()
    loads(1).wait()
    stream = tok[...].astype(F32)
    scale = lax.rsqrt(jnp.mean(stream * stream, axis=-1, keepdims=True) + EPSILON)
    normed = (stream * scale * again[...].reshape(1, -1).astype(F32)).astype(BF)
    loads(3).wait()
    q_send[...] = dot(normed, wq[...]).astype(BF).astype(F32)
    pl.semaphore_wait(barrier, n_tp - 1 + n_ep - 1)

    def q_copy(i):
        to = tp_peer(i)
        return pltpu.make_async_remote_copy(
            src_ref=q_send.at[pl.ds(to, 1)], dst_ref=q_recv.at[pl.ds(t, 1)],
            send_sem=q_ss, recv_sem=q_rs, device_id=(e, to), device_id_type=MESH,
        )

    @pl.loop(0, n_tp - 1)
    def _(i):
        q_copy(i).start()

    own = iota((rows, 1), 0) == t
    for i in (4, 5, 6, 7):
        loads(i).wait()

    def own_row(value):
        return jnp.sum(jnp.where(own, value, 0.0), axis=0, keepdims=True)

    key_new = own_row(dot(normed, wk[...])).astype(BF).astype(F32)
    value_new = own_row(dot(normed, wv[...])).astype(BF).astype(F32)
    eye = iota((HEADS, HEADS), 0) == iota((HEADS, HEADS), 1)
    bias = jnp.sum(jnp.where(eye, fb[...].reshape(1, -1), 0.0), axis=1, keepdims=True)
    gate_all = dot_t(wf[...], normed)
    own_lane = iota((1, rows), 1) == t
    gate_in = jnp.sum(jnp.where(own_lane, gate_all, 0.0), axis=1, keepdims=True) + bias
    log_gate = jnp.minimum(gate_in, 0.0) - jnp.log1p(jnp.exp(-jnp.abs(gate_in)))
    loads(11).wait()
    load_len.wait()
    length = len_ref[0]
    logcum = lc[0]
    position = iota((1, logcum.shape[1]), 1)
    latest = jnp.sum(jnp.where(position == length - 1, logcum, 0.0), axis=1, keepdims=True)

    for i in (12, 13, 14):
        loads(i).wait()
    eye_rows = iota((rows, rows), 0) == iota((rows, rows), 1)

    def column(row, zero):
        return jnp.sum(jnp.where(eye_rows, row, zero), axis=1, keepdims=True)

    chosen = rg[...].reshape(1, -1) * (n_ep // GROUPS) + re[...]
    slot_row = iota((picks, rows), 0)
    named = jnp.logical_or(
        chosen[0:1, :] == slot_row // SLOTS, chosen[1:2, :] == slot_row // SLOTS
    )
    named = named.astype(F32)
    before = (iota((rows, rows), 0) < iota((rows, rows), 1)).astype(F32).astype(BF)
    earlier = dot(named.astype(BF), before)
    place = jnp.where(earlier == (slot_row % SLOTS).astype(F32), named, 0.0).astype(BF)
    slot_lane = iota((rows, picks), 1)
    first = column(chosen[0:1, :], 0) == slot_lane // SLOTS
    second = column(chosen[1:2, :], 0) == slot_lane // SLOTS
    named_t = jnp.logical_or(first, second).astype(F32)
    before_t = (iota((rows, rows), 1) < iota((rows, rows), 0)).astype(F32).astype(BF)
    earlier_t = dot(before_t, named_t.astype(BF))
    here = earlier_t == (slot_lane % SLOTS).astype(F32)
    weight_t = jnp.where(first, column(rw[0:1, :], 0.0), column(rw[1:2, :], 0.0))
    combine = exact_parts(jnp.where(here, named_t * weight_t, 0.0))

    pltpu.make_async_copy(q_recv.at[pl.ds(0, n_tp - 1)], q_recv.at[pl.ds(0, n_tp - 1)], q_rs).wait()
    q16 = jnp.where(iota((n_tp, 1), 0) == t, q_send[...], q_recv[...])
    twice = (iota((HEADS, n_tp), 0) // 2 == iota((HEADS, n_tp), 1)).astype(F32).astype(BF)
    q32 = dot(twice, q16.astype(BF))
    turned = pltpu.roll(q32, HEAD, 1)
    odd = iota((HEADS, 2 * HEAD), 0) % 2 == 1
    low = iota((HEADS, 2 * HEAD), 1) < HEAD
    q_both = jnp.where(odd == low, turned, q32)
    q_wide = jnp.concatenate([q_both] * (KV_HEADS // 2), axis=1)
    kv_width = KV_HEADS * HEAD
    mine = iota((HEADS, kv_width), 1) // HEAD == iota((HEADS, kv_width), 0) // (HEADS // KV_HEADS)
    q_wide = jnp.where(mine, q_wide, 0.0)
    score_scale = HEAD ** (-0.5)
    own_score = jnp.sum(q_wide * key_new, axis=1, keepdims=True) * score_scale
    loads(9).wait()
    scores = dot_t(q_wide.astype(BF), ck[0]) * score_scale
    scores = scores + latest + log_gate - logcum
    usable = position < length
    scores = jnp.where(usable, scores, MASKED_SCORE)
    peak = jnp.maximum(jnp.max(scores, axis=1, keepdims=True), own_score)
    weights = jnp.where(usable, jnp.exp(scores - peak), 0.0)
    own_weight = jnp.exp(own_score - peak)
    denominator = jnp.sum(weights, axis=1, keepdims=True) + own_weight
    loads(10).wait()
    summed = dot(weights.astype(BF), cv[0])
    summed = summed + own_weight.astype(BF).astype(F32) * value_new
    summed = jnp.where(mine, summed, 0.0)
    folded = summed[:, : 2 * HEAD]
    for k in range(1, KV_HEADS // 2):
        folded = folded + summed[:, k * 2 * HEAD : (k + 1) * 2 * HEAD]
    folded = ((folded + pltpu.roll(folded, HEAD, 1)) / denominator).astype(BF)
    pair = iota((n_tp, HEADS), 1) - 2 * iota((n_tp, HEADS), 0)
    even_rows = dot((pair == 0).astype(F32).astype(BF), folded)
    odd_rows = dot((pair == 1).astype(F32).astype(BF), folded)
    att_all[t] = jnp.where(iota((n_tp, 2 * HEAD), 1) < HEAD, even_rows, odd_rows).astype(BF)

    def att_copy(i):
        return pltpu.make_async_remote_copy(
            src_ref=att_all.at[t], dst_ref=att_all.at[t],
            send_sem=a_ss, recv_sem=a_rs, device_id=(e, tp_peer(i)), device_id_type=MESH,
        )

    @pl.loop(0, n_tp - 1)
    def _(i):
        att_copy(i).start()

    residual = tok[:, pl.ds(pl.multiple_of(t * width, width), width)].astype(F32)
    loads(8).wait()
    pltpu.make_async_copy(
        att_all.at[pl.ds(0, n_tp - 1)], att_all.at[pl.ds(0, n_tp - 1)], a_rs
    ).wait()
    att_rows[...] = att_all[...].reshape(n_tp * n_tp, 2 * HEAD).astype(F32)
    attended = jnp.concatenate(
        [att_rows[pl.ds(k, n_tp, stride=n_tp), :].astype(BF) for k in range(n_tp)], axis=1
    )
    mixed = (residual + dot(attended, wo[...])).astype(BF)

    d_send[...] = dot(place, mixed).astype(BF)

    def pick_copy(i, src, dst, ss, rs):
        to = ep_peer(i)
        return pltpu.make_async_remote_copy(
            src_ref=src.at[pl.ds(pl.multiple_of(to * SLOTS, SLOTS), SLOTS)],
            dst_ref=dst.at[pl.ds(pl.multiple_of(e * SLOTS, SLOTS), SLOTS)],
            send_sem=ss, recv_sem=rs, device_id=(to, t), device_id_type=MESH,
        )

    def all_picks(ref, sem):
        part = ref.at[pl.ds(0, picks - SLOTS)]
        return pltpu.make_async_copy(part, part, sem)

    @pl.loop(0, n_ep - 1)
    def _(i):
        pick_copy(i, d_send, d_recv, d_ss, d_rs).start()

    own_slots = iota((picks, 1), 0) // SLOTS == e
    all_picks(d_recv, d_rs).wait()
    x_all[t] = jnp.where(own_slots, d_send[...].astype(F32), d_recv[...].astype(F32)).astype(BF)

    far_first = sorted(range(1, n_y), key=lambda d: -min(d, n_y - d))
    partner = 2 * y + 1 - c

    def column_copy(buf, d, ss, rs):
        to = 2 * lax.rem(y + d, n_y) + c
        return pltpu.make_async_remote_copy(
            src_ref=buf.at[t], dst_ref=buf.at[t],
            send_sem=ss.at[d], recv_sem=rs.at[d], device_id=(e, to), device_id_type=MESH,
        )

    def pass_on(buf, d, fs, ps):
        slot = 2 * lax.rem(y + n_y - d, n_y) + c
        return pltpu.make_async_remote_copy(
            src_ref=buf.at[slot], dst_ref=buf.at[slot],
            send_sem=fs.at[d], recv_sem=ps.at[d], device_id=(e, partner), device_id_type=MESH,
        )

    def gather(buf, ss, rs, fs, ps):
        for d in far_first:
            column_copy(buf, d, ss, rs).start()
        pass_on(buf, 0, fs, ps).start()
        for d in far_first[::-1]:
            column_copy(buf, d, ss, rs).wait_recv()
            pass_on(buf, d, fs, ps).start()
        for d in range(n_y):
            pass_on(buf, d, fs, ps).wait_recv()

    def gather_end(buf, ss, rs, fs, ps):
        for d in range(n_y):
            if d:
                column_copy(buf, d, ss, rs).wait_send()
            pass_on(buf, d, fs, ps).wait_send()

    gather(x_all, x_ss, x_rs, x_fs, x_ps)
    for i in (2, 15, 16, 17):
        loads(i).wait()
    total = jnp.zeros((picks, width), F32)
    for k in range(n_tp):
        part = x_all[k].astype(F32)
        total = total + part * part
    scale = lax.rsqrt(jnp.sum(total, axis=1, keepdims=True) / (n_tp * width) + EPSILON)
    gain = fgain[...].reshape(1, -1).astype(F32)
    moe_in = jnp.concatenate(
        [
            (x_all[k].astype(F32) * scale * gain[:, k * width : (k + 1) * width]).astype(BF)
            for k in range(n_tp)
        ],
        axis=1,
    )
    gated = dot(moe_in, wg[0])
    up = dot(moe_in, wu[0])
    h_all[t] = (gated / (1.0 + jnp.exp(-gated)) * up).astype(BF)
    gather(h_all, h_ss, h_rs, h_fs, h_ps)
    hidden = jnp.concatenate([h_all[k] for k in range(n_tp)], axis=1)
    r_send[...] = dot(hidden, wd[0]).astype(BF)

    @pl.loop(0, n_ep - 1)
    def _(i):
        pick_copy(i, r_send, r_recv, r_ss, r_rs).start()

    all_picks(r_recv, r_rs).wait()
    back = jnp.where(own_slots, r_send[...].astype(F32), r_recv[...].astype(F32)).astype(BF)
    moe_sum = sum(dot(part, back) for part in combine[::-1])
    out_ref[...] = (mixed.astype(F32) + moe_sum).astype(BF)

    pltpu.make_async_copy(q_send.at[pl.ds(0, n_tp - 1)], q_send.at[pl.ds(0, n_tp - 1)], q_ss).wait()
    pltpu.make_async_copy(
        att_all.at[pl.ds(0, n_tp - 1)], att_all.at[pl.ds(0, n_tp - 1)], a_ss
    ).wait()
    all_picks(d_send, d_ss).wait()
    gather_end(x_all, x_ss, x_rs, x_fs, x_ps)
    gather_end(h_all, h_ss, h_rs, h_fs, h_ps)
    all_picks(r_send, r_ss).wait()


def on_device(*args):
    args = list(args)
    for i in (6, 14, 15):
        args[i] = args[i].T
    n_ep = lax.axis_size("ep")
    n_tp = lax.axis_size("tp")
    rows = args[0].shape[0]
    width = args[8].shape[1]
    picks = n_ep * SLOTS
    any_spec = pl.BlockSpec(memory_space=pl.ANY)
    specs = [any_spec] * 19
    held = [pltpu.VMEM(a.shape, a.dtype) for i, a in enumerate(args) if i != 12]
    dma = pltpu.SemaphoreType.DMA
    n_y = n_tp // 2
    scratch = held + [
        pltpu.VMEM((rows, width), F32),
        pltpu.VMEM((n_tp, width), F32),
        pltpu.VMEM((n_tp, n_tp, 2 * HEAD), BF),
        pltpu.VMEM((n_tp * n_tp, 2 * HEAD), F32),
        pltpu.VMEM((picks, width), BF),
        pltpu.VMEM((picks, width), BF),
        pltpu.VMEM((n_tp, picks, width), BF),
        pltpu.VMEM((n_tp, picks, width), BF),
        pltpu.VMEM((picks, width), BF),
        pltpu.VMEM((picks, width), BF),
        dma((18,)),
        dma, dma, dma, dma, dma, dma,
        dma((n_y,)), dma((n_y,)), dma((n_y,)), dma((n_y,)),
        dma((n_y,)), dma((n_y,)), dma((n_y,)), dma((n_y,)),
        dma, dma, dma, pltpu.SMEM((1,), jnp.int32),
    ]
    return pl.pallas_call(
        functools.partial(layer_kernel, n_ep, n_tp),
        out_shape=jax.ShapeDtypeStruct((rows, width), BF),
        in_specs=specs,
        out_specs=pl.BlockSpec(memory_space=pltpu.VMEM),
        scratch_shapes=scratch,
        compiler_params=pltpu.CompilerParams(
            collective_id=0, has_side_effects=True, vmem_limit_bytes=60 * 1024 * 1024
        ),
        name="layer",
    )(*args)


def solution(mesh):
    placed = (
        P("ep", None),
        P(),
        P(),
        P(None, "tp"),
        P(),
        P(),
        P(),
        P(),
        P(None, "tp"),
        P(("ep", "tp"), None, None),
        P(("ep", "tp"), None, None),
        P(("ep", "tp"), None, None),
        P(("ep", "tp")),
        P("ep"),
        P("ep", None),
        P("ep", None),
        P("ep", None, "tp"),
        P("ep", None, "tp"),
        P("ep", None, "tp"),
    )
    return jax.shard_map(
        on_device, mesh=mesh, in_specs=placed, out_specs=P("ep", "tp"), check_vma=False
    )
```

```python
import functools

import jax
import jax.numpy as jnp
from jax import lax
from jax.experimental import pallas as pl
from jax.experimental.pallas import tpu as pltpu
from jax.sharding import PartitionSpec as P

HEADS = 32
KV_HEADS = 4
HEAD = 64
GROUPS = 4
EPSILON = 1e-06
MASKED_SCORE = -1e30
SLOTS = 2
BF = jnp.bfloat16
F32 = jnp.float32
MESH = pl.DeviceIdType.MESH


def iota(shape, dim):
    return lax.broadcasted_iota(jnp.int32, shape, dim)


def dot(a, b):
    return jnp.dot(a, b, preferred_element_type=F32)


def dot_t(a, b):
    return lax.dot_general(a, b, (((1,), (1,)), ((), ())), preferred_element_type=F32)


def exact_parts(x):
    a = x.astype(BF)
    r = x - a.astype(F32)
    b = r.astype(BF)
    return a, b, (r - b.astype(F32)).astype(BF)


def layer_kernel(n_ep, n_tp, bounds, *refs):
    inputs, out_ref, rest = refs[:19], refs[19], refs[20:]
    held, scratch = rest[:18], rest[18:]
    (tok, again, fgain, wq, wk, wv, wf, fb, wo, ck, cv, lc, rg, re, rw, wg, wu, wd) = held
    sources = inputs[:12] + inputs[13:]
    count = len(bounds) - 1
    scratch = list(scratch)

    def take(number):
        taken = scratch[:number]
        del scratch[:number]
        return taken

    q_send, q_recv, att_all, att_rows, d_send, d_recv, r_send, r_recv, len_ref = take(9)
    x_all, h_all = take(count), take(count)
    in_sem, len_sem, q_ss, q_rs, a_ss, a_rs, d_ss, d_rs, r_ss, r_rs, ready = take(11)
    x_sems, h_sems = take(count), take(count)
    e = lax.axis_index("ep")
    t = lax.axis_index("tp")
    n_y = n_tp // 2
    y, c = t // 2, t % 2
    rows = tok.shape[0]
    picks = n_ep * SLOTS
    width = wo.shape[1]

    def ep_peer(i):
        k = (i + 1) // 2
        return lax.rem(e + n_ep // 2 + k * (1 - 2 * (i % 2)) + n_ep, n_ep)

    def tp_peer(i):
        k = (i + 1) // 2
        return lax.rem(t + n_tp // 2 + k * (1 - 2 * (i % 2)) + n_tp, n_tp)

    def loads(i):
        return pltpu.make_async_copy(sources[i], held[i], in_sem.at[i])

    for i in (0, 1, 3):
        loads(i).start()
    load_len = pltpu.make_async_copy(inputs[12], len_ref, len_sem)

    barrier = pltpu.get_barrier_semaphore()

    @pl.loop(0, n_tp - 1)
    def _(i):
        pl.semaphore_signal(barrier, inc=1, device_id=(e, tp_peer(i)), device_id_type=MESH)

    @pl.loop(0, n_ep - 1 - e)
    def _(i):
        pl.semaphore_signal(barrier, inc=1, device_id=(n_ep - 1 - i, t), device_id_type=MESH)

    loads(0).wait()
    loads(1).wait()
    stream = tok[...].astype(F32)
    scale = lax.rsqrt(jnp.mean(stream * stream, axis=-1, keepdims=True) + EPSILON)
    normed = (stream * scale * again[...].reshape(1, -1).astype(F32)).astype(BF)
    loads(3).wait()
    for i in (4, 5, 6, 7, 11):
        loads(i).start()
    load_len.start()
    for i in (12, 13, 14, 9, 10, 8, 2, 15, 16, 17):
        loads(i).start()
    q_send[...] = dot(normed, wq[...]).astype(BF).astype(F32)
    pl.semaphore_wait(barrier, n_tp - 1 + e)

    def q_copy(i):
        to = tp_peer(i)
        return pltpu.make_async_remote_copy(
            src_ref=q_send.at[pl.ds(to, 1)], dst_ref=q_recv.at[pl.ds(t, 1)],
            send_sem=q_ss, recv_sem=q_rs, device_id=(e, to), device_id_type=MESH,
        )

    @pl.loop(0, n_tp - 1, unroll=True)
    def _(i):
        q_copy(i).start()

    @pl.loop(0, e)
    def _(i):
        pl.semaphore_signal(ready, inc=1, device_id=(i, t), device_id_type=MESH)

    own = iota((rows, 1), 0) == t
    for i in (4, 5, 6, 7):
        loads(i).wait()

    def own_row(value):
        return jnp.sum(jnp.where(own, value, 0.0), axis=0, keepdims=True)

    key_new = own_row(dot(normed, wk[...])).astype(BF).astype(F32)
    value_new = own_row(dot(normed, wv[...])).astype(BF).astype(F32)
    eye = iota((HEADS, HEADS), 0) == iota((HEADS, HEADS), 1)
    bias = jnp.sum(jnp.where(eye, fb[...].reshape(1, -1), 0.0), axis=1, keepdims=True)
    gate_all = dot_t(wf[...], normed)
    own_lane = iota((1, rows), 1) == t
    gate_in = jnp.sum(jnp.where(own_lane, gate_all, 0.0), axis=1, keepdims=True) + bias
    log_gate = jnp.minimum(gate_in, 0.0) - jnp.log1p(jnp.exp(-jnp.abs(gate_in)))
    loads(11).wait()
    load_len.wait()
    length = len_ref[0]
    logcum = lc[0]
    position = iota((1, logcum.shape[1]), 1)
    latest = jnp.sum(jnp.where(position == length - 1, logcum, 0.0), axis=1, keepdims=True)

    for i in (12, 13, 14):
        loads(i).wait()
    eye_rows = iota((rows, rows), 0) == iota((rows, rows), 1)

    def column(row, zero):
        return jnp.sum(jnp.where(eye_rows, row, zero), axis=1, keepdims=True)

    chosen = rg[...].reshape(1, -1) * (n_ep // GROUPS) + re[...]
    slot_row = iota((picks, rows), 0)
    named = jnp.logical_or(
        chosen[0:1, :] == slot_row // SLOTS, chosen[1:2, :] == slot_row // SLOTS
    )
    named = named.astype(F32)
    before = (iota((rows, rows), 0) < iota((rows, rows), 1)).astype(F32).astype(BF)
    earlier = dot(named.astype(BF), before)
    place = jnp.where(earlier == (slot_row % SLOTS).astype(F32), named, 0.0).astype(BF)
    slot_lane = iota((rows, picks), 1)
    first = column(chosen[0:1, :], 0) == slot_lane // SLOTS
    second = column(chosen[1:2, :], 0) == slot_lane // SLOTS
    named_t = jnp.logical_or(first, second).astype(F32)
    before_t = (iota((rows, rows), 1) < iota((rows, rows), 0)).astype(F32).astype(BF)
    earlier_t = dot(before_t, named_t.astype(BF))
    here = earlier_t == (slot_lane % SLOTS).astype(F32)
    weight_t = jnp.where(first, column(rw[0:1, :], 0.0), column(rw[1:2, :], 0.0))
    combine = exact_parts(jnp.where(here, named_t * weight_t, 0.0))

    pltpu.make_async_copy(q_recv.at[pl.ds(0, n_tp - 1)], q_recv.at[pl.ds(0, n_tp - 1)], q_rs).wait()
    q16 = jnp.where(iota((n_tp, 1), 0) == t, q_send[...], q_recv[...])
    twice = (iota((HEADS, n_tp), 0) // 2 == iota((HEADS, n_tp), 1)).astype(F32).astype(BF)
    q32 = dot(twice, q16.astype(BF))
    turned = pltpu.roll(q32, HEAD, 1)
    odd = iota((HEADS, 2 * HEAD), 0) % 2 == 1
    low = iota((HEADS, 2 * HEAD), 1) < HEAD
    q_both = jnp.where(odd == low, turned, q32)
    q_wide = jnp.concatenate([q_both] * (KV_HEADS // 2), axis=1)
    kv_width = KV_HEADS * HEAD
    mine = iota((HEADS, kv_width), 1) // HEAD == iota((HEADS, kv_width), 0) // (HEADS // KV_HEADS)
    q_wide = jnp.where(mine, q_wide, 0.0)
    score_scale = HEAD ** (-0.5)
    own_score = jnp.sum(q_wide * key_new, axis=1, keepdims=True) * score_scale
    loads(9).wait()
    scores = dot_t(q_wide.astype(BF), ck[0]) * score_scale
    scores = scores + latest + log_gate - logcum
    usable = position < length
    scores = jnp.where(usable, scores, MASKED_SCORE)
    peak = jnp.maximum(jnp.max(scores, axis=1, keepdims=True), own_score)
    weights = jnp.where(usable, jnp.exp(scores - peak), 0.0)
    own_weight = jnp.exp(own_score - peak)
    denominator = jnp.sum(weights, axis=1, keepdims=True) + own_weight
    loads(10).wait()
    summed = dot(weights.astype(BF), cv[0])
    summed = summed + own_weight.astype(BF).astype(F32) * value_new
    summed = jnp.where(mine, summed, 0.0)
    folded = summed[:, : 2 * HEAD]
    for k in range(1, KV_HEADS // 2):
        folded = folded + summed[:, k * 2 * HEAD : (k + 1) * 2 * HEAD]
    folded = ((folded + pltpu.roll(folded, HEAD, 1)) / denominator).astype(BF)
    pair = iota((n_tp, HEADS), 1) - 2 * iota((n_tp, HEADS), 0)
    even_rows = dot((pair == 0).astype(F32).astype(BF), folded)
    odd_rows = dot((pair == 1).astype(F32).astype(BF), folded)
    att_all[t] = jnp.where(iota((n_tp, 2 * HEAD), 1) < HEAD, even_rows, odd_rows).astype(BF)

    def att_copy(i):
        return pltpu.make_async_remote_copy(
            src_ref=att_all.at[t], dst_ref=att_all.at[t],
            send_sem=a_ss, recv_sem=a_rs, device_id=(e, tp_peer(i)), device_id_type=MESH,
        )

    @pl.loop(0, n_tp - 1, unroll=True)
    def _(i):
        att_copy(i).start()

    residual = tok[:, pl.ds(pl.multiple_of(t * width, width), width)].astype(F32)
    loads(8).wait()
    pltpu.make_async_copy(
        att_all.at[pl.ds(0, n_tp - 1)], att_all.at[pl.ds(0, n_tp - 1)], a_rs
    ).wait()
    att_rows[...] = att_all[...].reshape(n_tp * n_tp, 2 * HEAD).astype(F32)
    attended = jnp.concatenate(
        [att_rows[pl.ds(k, n_tp, stride=n_tp), :].astype(BF) for k in range(n_tp)], axis=1
    )
    mixed = (residual + dot(attended, wo[...])).astype(BF)

    d_send[...] = dot(place, mixed).astype(BF)

    @pl.when(e < n_ep - 1)
    def _():
        pl.semaphore_wait(ready, n_ep - 1 - e)

    def pick_copy(to, src, dst, ss, rs):
        return pltpu.make_async_remote_copy(
            src_ref=src.at[pl.ds(pl.multiple_of(to * SLOTS, SLOTS), SLOTS)],
            dst_ref=dst.at[pl.ds(pl.multiple_of(e * SLOTS, SLOTS), SLOTS)],
            send_sem=ss, recv_sem=rs, device_id=(to, t), device_id_type=MESH,
        )

    def slots_wait(ref, sem, count):
        part = ref.at[pl.ds(0, count * SLOTS)]
        return pltpu.make_async_copy(part, part, sem).wait()

    batch = sum((e >= first).astype(jnp.int32) for first in bounds[1:-1])

    @pl.loop(0, n_ep - 1, unroll=True)
    def _(i):
        pick_copy(ep_peer(i), d_send, d_recv, d_ss, d_rs.at[batch]).start()

    own_slots = iota((picks, 1), 0) // SLOTS == e
    far_first = sorted(range(1, n_y), key=lambda d: -min(d, n_y - d))
    partner = 2 * y + 1 - c

    def column_copy(buf, d, sems):
        to = 2 * lax.rem(y + d, n_y) + c
        return pltpu.make_async_remote_copy(
            src_ref=buf.at[t], dst_ref=buf.at[t],
            send_sem=sems.at[0, d], recv_sem=sems.at[1, d], device_id=(e, to), device_id_type=MESH,
        )

    def pass_on(buf, d, sems):
        slot = 2 * lax.rem(y + n_y - d, n_y) + c
        return pltpu.make_async_remote_copy(
            src_ref=buf.at[slot], dst_ref=buf.at[slot],
            send_sem=sems.at[2, d], recv_sem=sems.at[3, d], device_id=(e, partner), device_id_type=MESH,
        )

    def gather_start(buf, sems):
        for d in far_first:
            column_copy(buf, d, sems).start()
        pass_on(buf, 0, sems).start()

    def gather_pass(buf, sems):
        for d in far_first[::-1]:
            column_copy(buf, d, sems).wait_recv()
            pass_on(buf, d, sems).start()

    def gather_finish(buf, sems):
        for d in range(n_y):
            pass_on(buf, d, sems).wait_recv()

    def gather_end(buf, sems):
        for d in range(n_y):
            if d:
                column_copy(buf, d, sems).wait_send()
            pass_on(buf, d, sems).wait_send()

    def arrive(k):
        count = bounds[k + 1] - bounds[k]
        slots = slice(bounds[k] * SLOTS, bounds[k + 1] * SLOTS)

        @pl.when(batch == k)
        def _():
            slots_wait(d_recv, d_rs.at[k], count - 1)

        @pl.when(batch != k)
        def _():
            slots_wait(d_recv, d_rs.at[k], count)

        x_all[k][t] = jnp.where(
            own_slots[slots], d_send[slots, :].astype(F32), d_recv[slots, :].astype(F32)
        ).astype(BF)
        gather_start(x_all[k], x_sems[k])

    def expand(k):
        gather_finish(x_all[k], x_sems[k])
        if k == 0:
            for i in (2, 15, 16, 17):
                loads(i).wait()
        buf = x_all[k]
        total = jnp.zeros(buf.shape[1:], F32)
        for j in range(n_tp):
            part = buf[j].astype(F32)
            total = total + part * part
        scale = lax.rsqrt(jnp.sum(total, axis=1, keepdims=True) / (n_tp * width) + EPSILON)
        gain = fgain[...].reshape(1, -1).astype(F32)
        moe_in = jnp.concatenate(
            [
                (buf[j].astype(F32) * scale * gain[:, j * width : (j + 1) * width]).astype(BF)
                for j in range(n_tp)
            ],
            axis=1,
        )
        gated = dot(moe_in, wg[0])
        up = dot(moe_in, wu[0])
        h_all[k][t] = (gated / (1.0 + jnp.exp(-gated)) * up).astype(BF)
        gather_start(h_all[k], h_sems[k])

    def contract(k):
        slots = slice(bounds[k] * SLOTS, bounds[k + 1] * SLOTS)
        gather_finish(h_all[k], h_sems[k])
        hidden = jnp.concatenate([h_all[k][j] for j in range(n_tp)], axis=1)
        r_send[slots, :] = dot(hidden, wd[0]).astype(BF)

        @pl.loop(0, n_ep - 1, unroll=True)
        def _(i):
            to = ep_peer(i)

            @pl.when(jnp.logical_and(to >= bounds[k], to < bounds[k + 1]))
            def _():
                pick_copy(to, r_send, r_recv, r_ss, r_rs).start()

    n_batches = len(bounds) - 1
    arrive(0)
    gather_pass(x_all[0], x_sems[0])
    expand(0)
    for k in range(1, n_batches):
        arrive(k)
        gather_pass(h_all[k - 1], h_sems[k - 1])
        gather_pass(x_all[k], x_sems[k])
        contract(k - 1)
        expand(k)
    gather_pass(h_all[n_batches - 1], h_sems[n_batches - 1])
    contract(n_batches - 1)

    slots_wait(r_recv, r_rs, n_ep - 1)
    back = jnp.where(own_slots, r_send[...].astype(F32), r_recv[...].astype(F32)).astype(BF)
    moe_sum = sum(dot(part, back) for part in combine[::-1])
    out_ref[...] = mixed.astype(F32) + moe_sum

    pltpu.make_async_copy(q_send.at[pl.ds(0, n_tp - 1)], q_send.at[pl.ds(0, n_tp - 1)], q_ss).wait()
    pltpu.make_async_copy(
        att_all.at[pl.ds(0, n_tp - 1)], att_all.at[pl.ds(0, n_tp - 1)], a_ss
    ).wait()
    slots_wait(d_send, d_ss, n_ep - 1)
    for k in range(n_batches):
        gather_end(x_all[k], x_sems[k])
        gather_end(h_all[k], h_sems[k])
    slots_wait(r_send, r_ss, n_ep - 1)


def batch_bounds(n_ep):
    return (0, n_ep // 3, n_ep)


def on_device(*args):
    args = list(args)
    for i in (6, 14, 15):
        args[i] = args[i].T
    n_ep = lax.axis_size("ep")
    n_tp = lax.axis_size("tp")
    rows = args[0].shape[0]
    width = args[8].shape[1]
    picks = n_ep * SLOTS
    bounds = batch_bounds(n_ep)
    sizes = [(b - a) * SLOTS for a, b in zip(bounds, bounds[1:])]
    any_spec = pl.BlockSpec(memory_space=pltpu.HBM)
    specs = [any_spec] * 19
    held = [pltpu.VMEM(a.shape, a.dtype) for i, a in enumerate(args) if i != 12]
    dma = pltpu.SemaphoreType.DMA
    scratch = held + [
        pltpu.VMEM((rows, width), F32),
        pltpu.VMEM((n_tp, width), F32),
        pltpu.VMEM((n_tp, n_tp, 2 * HEAD), BF),
        pltpu.VMEM((n_tp * n_tp, 2 * HEAD), F32),
        pltpu.VMEM((picks, width), BF),
        pltpu.VMEM((picks, width), BF),
        pltpu.VMEM((picks, width), BF),
        pltpu.VMEM((picks, width), BF),
        pltpu.SMEM((1,), jnp.int32),
    ]
    scratch += [pltpu.VMEM((n_tp, size, width), BF) for size in sizes + sizes]
    scratch += [dma((18,)), dma, dma, dma, dma, dma, dma, dma((len(sizes),)), dma, dma]
    scratch += [pltpu.SemaphoreType.REGULAR]
    scratch += [dma((4, n_tp // 2)) for _ in sizes + sizes]
    args = [
        a if i == 12 else pltpu.with_memory_space_constraint(a, pltpu.HBM)
        for i, a in enumerate(args)
    ]
    return pl.pallas_call(
        functools.partial(layer_kernel, n_ep, n_tp, bounds),
        out_shape=jax.ShapeDtypeStruct((rows, width), F32),
        in_specs=specs,
        out_specs=pl.BlockSpec(memory_space=pltpu.VMEM),
        scratch_shapes=scratch,
        compiler_params=pltpu.CompilerParams(
            collective_id=0, has_side_effects=True, vmem_limit_bytes=24 * 1024 * 1024
        ),
        name="layer",
    )(*args).astype(BF)


def solution(mesh):
    placed = (
        P("ep", None),
        P(),
        P(),
        P(None, "tp"),
        P(),
        P(),
        P(),
        P(),
        P(None, "tp"),
        P(("ep", "tp"), None, None),
        P(("ep", "tp"), None, None),
        P(("ep", "tp"), None, None),
        P(("ep", "tp")),
        P("ep"),
        P("ep", None),
        P("ep", None),
        P("ep", None, "tp"),
        P("ep", None, "tp"),
        P("ep", None, "tp"),
    )
    return jax.shard_map(
        on_device, mesh=mesh, in_specs=placed, out_specs=P("ep", "tp"), check_vma=False
    )
```

```python
import functools

import jax
import jax.numpy as jnp
from jax import lax
from jax.experimental import pallas as pl
from jax.experimental.pallas import tpu as pltpu
from jax.sharding import PartitionSpec as P

HEADS = 32
KV_HEADS = 4
HEAD = 64
GROUPS = 4
EPSILON = 1e-06
MASKED_SCORE = -1e30
SLOTS = 2
BF = jnp.bfloat16
F32 = jnp.float32
MESH = pl.DeviceIdType.MESH


def iota(shape, dim):
    return lax.broadcasted_iota(jnp.int32, shape, dim)


def dot(a, b):
    return jnp.dot(a, b, preferred_element_type=F32)


def dot_t(a, b):
    return lax.dot_general(a, b, (((1,), (1,)), ((), ())), preferred_element_type=F32)


def exact_parts(x):
    a = x.astype(BF)
    r = x - a.astype(F32)
    b = r.astype(BF)
    return a, b, (r - b.astype(F32)).astype(BF)


def layer_kernel(n_ep, n_tp, bounds, orders, *refs):
    inputs, out_ref, rest = refs[:19], refs[19], refs[20:]
    held, scratch = rest[:18], rest[18:]
    (tok, again, fgain, wq, wk, wv, wf, fb, wo, ck, cv, lc, rg, re, rw, wg, wu, wd) = held
    sources = inputs[:12] + inputs[13:]
    count = len(bounds) - 1
    scratch = list(scratch)

    def take(number):
        taken = scratch[:number]
        del scratch[:number]
        return taken

    q_send, q_recv, att_all, att_rows, d_send, d_recv, r_send, r_recv, len_ref = take(9)
    x_all, h_all = take(count), take(count)
    in_sem, len_sem, q_ss, q_rs, a_ss, a_rs, d_ss, d_rs, r_ss, r_rs, ready = take(11)
    x_sems = list(zip(take(count), take(count)))
    h_sems = list(zip(take(count), take(count)))
    ep = lax.axis_index("ep")
    zero_rank = n_ep // 3 - 1

    def rank_of(place):
        return jnp.where(place == 0, zero_rank, place - (place <= zero_rank).astype(jnp.int32))

    e = rank_of(ep)
    t = lax.axis_index("tp")
    n_y = n_tp // 2
    y, c = t // 2, t % 2
    rows = tok.shape[0]
    late = n_ep * 2 // 3
    picks = n_ep * SLOTS
    width = wo.shape[1]

    def at_rank(rank):
        return jnp.where(rank == zero_rank, 0, rank + (rank < zero_rank).astype(jnp.int32))

    def tp_peer(i):
        k = (i + 1) // 2
        return lax.rem(t + n_tp // 2 + k * (1 - 2 * (i % 2)) + n_tp, n_tp)

    def loads(i):
        return pltpu.make_async_copy(sources[i], held[i], in_sem.at[i])

    for i in (0, 1, 3):
        loads(i).start()
    load_len = pltpu.make_async_copy(inputs[12], len_ref, len_sem)

    barrier = pltpu.get_barrier_semaphore()

    @pl.loop(0, n_tp - 1)
    def _(i):
        pl.semaphore_signal(barrier, inc=1, device_id=(ep, tp_peer(i)), device_id_type=MESH)

    @pl.loop(0, n_ep - 1 - e)
    def _(i):
        pl.semaphore_signal(barrier, inc=1, device_id=(at_rank(n_ep - 1 - i), t), device_id_type=MESH)

    loads(0).wait()
    loads(1).wait()
    stream = tok[...].astype(F32)
    scale = lax.rsqrt(jnp.mean(stream * stream, axis=-1, keepdims=True) + EPSILON)
    normed = (stream * scale * again[...].reshape(1, -1).astype(F32)).astype(BF)
    loads(3).wait()
    for i in (4, 5, 6, 7, 11):
        loads(i).start()
    load_len.start()
    for i in (12, 13, 14, 9, 10, 8, 2, 15, 16, 17):
        loads(i).start()
    q_send[...] = dot(normed, wq[...]).astype(BF).astype(F32)
    pl.semaphore_wait(barrier, n_tp - 1 + e)

    def q_copy(i):
        to = tp_peer(i)
        return pltpu.make_async_remote_copy(
            src_ref=q_send.at[pl.ds(to, 1)], dst_ref=q_recv.at[pl.ds(t, 1)],
            send_sem=q_ss, recv_sem=q_rs, device_id=(ep, to), device_id_type=MESH,
        )

    @pl.loop(0, n_tp - 1, unroll=True)
    def _(i):
        q_copy(i).start()

    late_one = (e >= late).astype(jnp.int32)

    @pl.loop(0, e)
    def _(i):
        pl.semaphore_signal(
            ready.at[late_one], inc=1, device_id=(at_rank(i), t), device_id_type=MESH
        )

    own = iota((rows, 1), 0) == t
    for i in (4, 5, 6, 7):
        loads(i).wait()

    def own_row(value):
        return jnp.sum(jnp.where(own, value, 0.0), axis=0, keepdims=True)

    key_new = own_row(dot(normed, wk[...])).astype(BF).astype(F32)
    value_new = own_row(dot(normed, wv[...])).astype(BF).astype(F32)
    eye = iota((HEADS, HEADS), 0) == iota((HEADS, HEADS), 1)
    bias = jnp.sum(jnp.where(eye, fb[...].reshape(1, -1), 0.0), axis=1, keepdims=True)
    gate_all = dot_t(wf[...], normed)
    own_lane = iota((1, rows), 1) == t
    gate_in = jnp.sum(jnp.where(own_lane, gate_all, 0.0), axis=1, keepdims=True) + bias
    log_gate = jnp.minimum(gate_in, 0.0) - jnp.log1p(jnp.exp(-jnp.abs(gate_in)))
    loads(11).wait()
    load_len.wait()
    length = len_ref[0]
    logcum = lc[0]
    position = iota((1, logcum.shape[1]), 1)
    latest = jnp.sum(jnp.where(position == length - 1, logcum, 0.0), axis=1, keepdims=True)

    for i in (12, 13, 14):
        loads(i).wait()
    eye_rows = iota((rows, rows), 0) == iota((rows, rows), 1)

    def column(row, zero):
        return jnp.sum(jnp.where(eye_rows, row, zero), axis=1, keepdims=True)

    chosen = rg[...].reshape(1, -1) * (n_ep // GROUPS) + re[...]
    chosen = rank_of(chosen)
    slot_row = iota((picks, rows), 0)
    named = jnp.logical_or(
        chosen[0:1, :] == slot_row // SLOTS, chosen[1:2, :] == slot_row // SLOTS
    )
    named = named.astype(F32)
    before = (iota((rows, rows), 0) < iota((rows, rows), 1)).astype(F32).astype(BF)
    earlier = dot(named.astype(BF), before)
    place = jnp.where(earlier == (slot_row % SLOTS).astype(F32), named, 0.0).astype(BF)
    slot_lane = iota((rows, picks), 1)
    first = column(chosen[0:1, :], 0) == slot_lane // SLOTS
    second = column(chosen[1:2, :], 0) == slot_lane // SLOTS
    named_t = jnp.logical_or(first, second).astype(F32)
    before_t = (iota((rows, rows), 1) < iota((rows, rows), 0)).astype(F32).astype(BF)
    earlier_t = dot(before_t, named_t.astype(BF))
    here = earlier_t == (slot_lane % SLOTS).astype(F32)
    weight_t = jnp.where(first, column(rw[0:1, :], 0.0), column(rw[1:2, :], 0.0))
    combine = exact_parts(jnp.where(here, named_t * weight_t, 0.0))

    pltpu.make_async_copy(q_recv.at[pl.ds(0, n_tp - 1)], q_recv.at[pl.ds(0, n_tp - 1)], q_rs).wait()
    q16 = jnp.where(iota((n_tp, 1), 0) == t, q_send[...], q_recv[...])
    twice = (iota((HEADS, n_tp), 0) // 2 == iota((HEADS, n_tp), 1)).astype(F32).astype(BF)
    q32 = dot(twice, q16.astype(BF))
    turned = pltpu.roll(q32, HEAD, 1)
    odd = iota((HEADS, 2 * HEAD), 0) % 2 == 1
    low = iota((HEADS, 2 * HEAD), 1) < HEAD
    q_both = jnp.where(odd == low, turned, q32)
    q_wide = jnp.concatenate([q_both] * (KV_HEADS // 2), axis=1)
    kv_width = KV_HEADS * HEAD
    mine = iota((HEADS, kv_width), 1) // HEAD == iota((HEADS, kv_width), 0) // (HEADS // KV_HEADS)
    q_wide = jnp.where(mine, q_wide, 0.0)
    score_scale = HEAD ** (-0.5)
    own_score = jnp.sum(q_wide * key_new, axis=1, keepdims=True) * score_scale
    loads(9).wait()
    scores = dot_t(q_wide.astype(BF), ck[0]) * score_scale
    scores = scores + latest + log_gate - logcum
    usable = position < length
    scores = jnp.where(usable, scores, MASKED_SCORE)
    peak = jnp.maximum(jnp.max(scores, axis=1, keepdims=True), own_score)
    weights = jnp.where(usable, jnp.exp(scores - peak), 0.0)
    own_weight = jnp.exp(own_score - peak)
    denominator = jnp.sum(weights, axis=1, keepdims=True) + own_weight
    loads(10).wait()
    summed = dot(weights.astype(BF), cv[0])
    summed = summed + own_weight.astype(BF).astype(F32) * value_new
    summed = jnp.where(mine, summed, 0.0)
    folded = summed[:, : 2 * HEAD]
    for k in range(1, KV_HEADS // 2):
        folded = folded + summed[:, k * 2 * HEAD : (k + 1) * 2 * HEAD]
    folded = ((folded + pltpu.roll(folded, HEAD, 1)) / denominator).astype(BF)
    pair = iota((n_tp, HEADS), 1) - 2 * iota((n_tp, HEADS), 0)
    even_rows = dot((pair == 0).astype(F32).astype(BF), folded)
    odd_rows = dot((pair == 1).astype(F32).astype(BF), folded)
    att_all[t] = jnp.where(iota((n_tp, 2 * HEAD), 1) < HEAD, even_rows, odd_rows).astype(BF)

    def att_copy(i):
        return pltpu.make_async_remote_copy(
            src_ref=att_all.at[t], dst_ref=att_all.at[t],
            send_sem=a_ss, recv_sem=a_rs, device_id=(ep, tp_peer(i)), device_id_type=MESH,
        )

    @pl.loop(0, n_tp - 1, unroll=True)
    def _(i):
        att_copy(i).start()

    residual = tok[:, pl.ds(pl.multiple_of(t * width, width), width)].astype(F32)
    loads(8).wait()
    pltpu.make_async_copy(
        att_all.at[pl.ds(0, n_tp - 1)], att_all.at[pl.ds(0, n_tp - 1)], a_rs
    ).wait()
    att_rows[...] = att_all[...].reshape(n_tp * n_tp, 2 * HEAD).astype(F32)
    attended = jnp.concatenate(
        [att_rows[pl.ds(k, n_tp, stride=n_tp), :].astype(BF) for k in range(n_tp)], axis=1
    )
    mixed = (residual + dot(attended, wo[...])).astype(BF)

    d_send[...] = dot(place, mixed).astype(BF)

    def pick_copy(to, src, dst, ss, rs):
        return pltpu.make_async_remote_copy(
            src_ref=src.at[pl.ds(pl.multiple_of(to * SLOTS, SLOTS), SLOTS)],
            dst_ref=dst.at[pl.ds(pl.multiple_of(e * SLOTS, SLOTS), SLOTS)],
            send_sem=ss, recv_sem=rs, device_id=(at_rank(to), t), device_id_type=MESH,
        )

    def slots_wait(ref, sem, count):
        part = ref.at[pl.ds(0, count * SLOTS)]
        return pltpu.make_async_copy(part, part, sem).wait()

    batch = sum((e >= first).astype(jnp.int32) for first in bounds[1:-1])

    def send_picks(first, last):
        @pl.loop(first, last, unroll=True)
        def _(i):
            to = i + (i >= e).astype(jnp.int32)
            pick_copy(to, d_send, d_recv, d_ss, d_rs.at[batch]).start()

    @pl.when(e < late - 1)
    def _():
        pl.semaphore_wait(ready.at[0], late - 1 - e)

    send_picks(0, late - 1)

    @pl.when(e < n_ep - 1)
    def _():
        pl.semaphore_wait(ready.at[1], jnp.minimum(n_ep - late, n_ep - 1 - e))

    send_picks(late - 1, n_ep - 1)

    own_slots = iota((picks, 1), 0) // SLOTS == e
    far_first = sorted(range(1, n_y), key=lambda d: -min(d, n_y - d))
    partner = 2 * y + 1 - c

    def column_copy(buf, d, sems):
        to = 2 * lax.rem(y + d, n_y) + 1 - c
        return pltpu.make_async_remote_copy(
            src_ref=buf.at[t], dst_ref=buf.at[t], send_sem=sems[0].at[0],
            recv_sem=sems[1].at[d - 1], device_id=(ep, to), device_id_type=MESH,
        )

    def pass_on(buf, d, sems):
        slot = 2 * lax.rem(y + n_y - d, n_y) + (c if d == 0 else 1 - c)
        return pltpu.make_async_remote_copy(
            src_ref=buf.at[slot], dst_ref=buf.at[slot], send_sem=sems[0].at[1],
            recv_sem=sems[0].at[2], device_id=(ep, partner), device_id_type=MESH,
        )

    def wait_parts(buf, count, sem):
        part = buf.at[pl.ds(0, count)]
        pltpu.make_async_copy(part, part, sem).wait()

    def gather_start(buf, sems):
        for d in far_first:
            column_copy(buf, d, sems).start()
        pass_on(buf, 0, sems).start()

    def gather_pass(buf, sems):
        for d in far_first[::-1]:
            column_copy(buf, d, sems).wait_recv()
            pass_on(buf, d, sems).start()

    def gather_finish(buf, sems):
        wait_parts(buf, n_y, sems[0].at[2])

    def gather_end(buf, sems):
        wait_parts(buf, n_y - 1, sems[0].at[0])
        wait_parts(buf, n_y, sems[0].at[1])

    def arrive(k):
        count = bounds[k + 1] - bounds[k]
        slots = slice(bounds[k] * SLOTS, bounds[k + 1] * SLOTS)

        @pl.when(batch == k)
        def _():
            slots_wait(d_recv, d_rs.at[k], count - 1)

        @pl.when(batch != k)
        def _():
            slots_wait(d_recv, d_rs.at[k], count)

        x_all[k][t] = jnp.where(
            own_slots[slots], d_send[slots, :].astype(F32), d_recv[slots, :].astype(F32)
        ).astype(BF)
        gather_start(x_all[k], x_sems[k])

    def expand(k):
        gather_finish(x_all[k], x_sems[k])
        buf = x_all[k]
        total = jnp.zeros(buf.shape[1:], F32)
        for j in range(n_tp):
            part = buf[j].astype(F32)
            total = total + part * part
        scale = lax.rsqrt(jnp.sum(total, axis=1, keepdims=True) / (n_tp * width) + EPSILON)
        gain = fgain[...].reshape(1, -1).astype(F32)
        moe_in = jnp.concatenate(
            [
                (buf[j].astype(F32) * scale * gain[:, j * width : (j + 1) * width]).astype(BF)
                for j in range(n_tp)
            ],
            axis=1,
        )
        gated = dot(moe_in, wg[0])
        up = dot(moe_in, wu[0])
        h_all[k][t] = (gated / (1.0 + jnp.exp(-gated)) * up).astype(BF)
        gather_start(h_all[k], h_sems[k])

    def contract(k):
        slots = slice(bounds[k] * SLOTS, bounds[k + 1] * SLOTS)
        gather_finish(h_all[k], h_sems[k])
        hidden = jnp.concatenate([h_all[k][j] for j in range(n_tp)], axis=1)
        r_send[slots, :] = dot(hidden, wd[0]).astype(BF)

        @pl.loop(bounds[k], bounds[k + 1], unroll=True)
        def _(to):
            @pl.when(to != e)
            def _():
                pick_copy(to, r_send, r_recv, r_ss, r_rs).start()

    n_batches = len(bounds) - 1

    def work(order):
        passed = set()

        def once(kind, k):
            if (kind, k) not in passed:
                passed.add((kind, k))
                if kind == "x":
                    gather_pass(x_all[k], x_sems[k])
                else:
                    gather_pass(h_all[k], h_sems[k])

        for step in order.split():
            kind, k = step[0], int(step[1])
            if kind == "a":
                arrive(k)
            elif kind == "p":
                once("x", k)
            elif kind == "q":
                once("h", k)
            elif kind == "x":
                once("x", k)
                expand(k)
            else:
                once("h", k)
                contract(k)

    for i in (2, 15, 16, 17):
        loads(i).wait()
    turn = jnp.where(e == zero_rank, 0, e)
    for low, high, order in orders:
        @pl.when(jnp.logical_and(turn >= low, turn < high))
        def _(order=order):
            work(order)

    slots_wait(r_recv, r_rs, n_ep - 1)
    back = jnp.where(own_slots, r_send[...].astype(F32), r_recv[...].astype(F32)).astype(BF)
    moe_sum = sum(dot(part, back) for part in combine[::-1])
    out_ref[...] = mixed.astype(F32) + moe_sum

    pltpu.make_async_copy(q_send.at[pl.ds(0, n_tp - 1)], q_send.at[pl.ds(0, n_tp - 1)], q_ss).wait()
    pltpu.make_async_copy(
        att_all.at[pl.ds(0, n_tp - 1)], att_all.at[pl.ds(0, n_tp - 1)], a_ss
    ).wait()
    slots_wait(d_send, d_ss, n_ep - 1)
    for k in range(n_batches):
        gather_end(x_all[k], x_sems[k])
        gather_end(h_all[k], h_sems[k])
    slots_wait(r_send, r_ss, n_ep - 1)


def batch_bounds(n_ep):
    return (0, n_ep // 3 - 1, n_ep * 2 // 3, n_ep)


def plan_orders(n_ep):
    early, late = n_ep // 3 - 1, n_ep * 2 // 3
    return (
        (0, early, "a0 x0 a1 a2 q0 p1 x1 p2 x2 h0 h1 h2"),
        (early, late, "a0 x0 a1 q0 p1 a2 h0 x1 p2 x2 h1 h2"),
        (late, n_ep, "a0 a1 a2 x0 x1 x2 h0 h1 h2"),
    )


def on_device(*args):
    args = list(args)
    for i in (6, 14, 15):
        args[i] = args[i].T
    n_ep = lax.axis_size("ep")
    n_tp = lax.axis_size("tp")
    rows = args[0].shape[0]
    width = args[8].shape[1]
    picks = n_ep * SLOTS
    bounds = batch_bounds(n_ep)
    sizes = [(b - a) * SLOTS for a, b in zip(bounds, bounds[1:])]
    any_spec = pl.BlockSpec(memory_space=pltpu.HBM)
    specs = [any_spec] * 19
    held = [pltpu.VMEM(a.shape, a.dtype) for i, a in enumerate(args) if i != 12]
    dma = pltpu.SemaphoreType.DMA
    scratch = held + [
        pltpu.VMEM((rows, width), F32),
        pltpu.VMEM((n_tp, width), F32),
        pltpu.VMEM((n_tp, n_tp, 2 * HEAD), BF),
        pltpu.VMEM((n_tp * n_tp, 2 * HEAD), F32),
        pltpu.VMEM((picks, width), BF),
        pltpu.VMEM((picks, width), BF),
        pltpu.VMEM((picks, width), BF),
        pltpu.VMEM((picks, width), BF),
        pltpu.SMEM((1,), jnp.int32),
    ]
    scratch += [pltpu.VMEM((n_tp, size, width), BF) for size in sizes + sizes]
    scratch += [dma((18,)), dma, dma, dma, dma, dma, dma, dma((len(sizes),)), dma, dma]
    scratch += [pltpu.SemaphoreType.REGULAR((2,))]
    for _ in range(2):
        scratch += [dma((3,)) for _ in sizes] + [dma((n_tp // 2 - 1,)) for _ in sizes]
    args = [
        a if i == 12 else pltpu.with_memory_space_constraint(a, pltpu.HBM)
        for i, a in enumerate(args)
    ]
    return pl.pallas_call(
        functools.partial(layer_kernel, n_ep, n_tp, bounds, plan_orders(n_ep)),
        out_shape=jax.ShapeDtypeStruct((rows, width), F32),
        in_specs=specs,
        out_specs=pl.BlockSpec(memory_space=pltpu.VMEM),
        scratch_shapes=scratch,
        compiler_params=pltpu.CompilerParams(
            collective_id=0, has_side_effects=True, vmem_limit_bytes=24 * 1024 * 1024
        ),
        name="layer",
    )(*args).astype(BF)


def solution(mesh):
    placed = (
        P("ep", None),
        P(),
        P(),
        P(None, "tp"),
        P(),
        P(),
        P(),
        P(),
        P(None, "tp"),
        P(("ep", "tp"), None, None),
        P(("ep", "tp"), None, None),
        P(("ep", "tp"), None, None),
        P(("ep", "tp")),
        P("ep"),
        P("ep", None),
        P("ep", None),
        P("ep", None, "tp"),
        P("ep", None, "tp"),
        P("ep", None, "tp"),
    )
    return jax.shard_map(
        on_device, mesh=mesh, in_specs=placed, out_specs=P("ep", "tp"), check_vma=False
    )
```

```python
import functools

import jax
import jax.numpy as jnp
from jax import lax
from jax.experimental import pallas as pl
from jax.experimental.pallas import tpu as pltpu
from jax.sharding import PartitionSpec as P

HEADS = 32
KV_HEADS = 4
HEAD = 64
GROUPS = 4
EPSILON = 1e-06
MASKED_SCORE = -1e30
SLOTS = 2
BF = jnp.bfloat16
F32 = jnp.float32
MESH = pl.DeviceIdType.MESH


def iota(shape, dim):
    return lax.broadcasted_iota(jnp.int32, shape, dim)


def dot(a, b):
    return jnp.dot(a, b, preferred_element_type=F32)


def dot_t(a, b):
    return lax.dot_general(a, b, (((1,), (1,)), ((), ())), preferred_element_type=F32)


def exact_parts(x):
    a = x.astype(BF)
    r = x - a.astype(F32)
    b = r.astype(BF)
    return a, b, (r - b.astype(F32)).astype(BF)


def layer_kernel(n_ep, n_tp, bounds, orders, *refs):
    inputs, out_ref, rest = refs[:19], refs[19], refs[20:]
    held, scratch = rest[:18], rest[18:]
    (tok, again, fgain, wq, wk, wv, wf, fb, wo, ck, cv, lc, rg, re, rw, wg, wu, wd) = held
    sources = inputs[:12] + inputs[13:]
    count = len(bounds) - 1
    scratch = list(scratch)

    def take(number):
        taken = scratch[:number]
        del scratch[:number]
        return taken

    q_send, q_recv, att_all, att_rows, d_send, d_recv, r_send, r_recv, decay, len_ref = take(10)
    x_all, h_all = take(count), take(count)
    in_sem, len_sem, q_ss, q_rs, a_ss, a_rs, d_ss, d_rs, r_ss, r_rs, ready = take(11)
    x_sems = list(zip(take(count), take(count)))
    h_sems = list(zip(take(count), take(count)))
    ep = lax.axis_index("ep")
    zero_rank = n_ep // 3 - 1

    def rank_of(place):
        return jnp.where(place == 0, zero_rank, place - (place <= zero_rank).astype(jnp.int32))

    e = rank_of(ep)
    t = lax.axis_index("tp")
    n_y = n_tp // 2
    y, c = t // 2, t % 2
    rows = tok.shape[0]
    late = n_ep * 2 // 3
    picks = n_ep * SLOTS
    width = wo.shape[1]

    def at_rank(rank):
        return jnp.where(rank == zero_rank, 0, rank + (rank < zero_rank).astype(jnp.int32))

    def tp_peer(i):
        k = (i + 1) // 2
        return lax.rem(t + n_tp // 2 + k * (1 - 2 * (i % 2)) + n_tp, n_tp)

    def loads(i):
        return pltpu.make_async_copy(sources[i], held[i], in_sem.at[i])

    for i in (0, 1, 3):
        loads(i).start()
    load_len = pltpu.make_async_copy(inputs[12], len_ref, len_sem)

    barrier = pltpu.get_barrier_semaphore()

    @pl.loop(0, n_tp - 1)
    def _(i):
        pl.semaphore_signal(barrier, inc=1, device_id=(ep, tp_peer(i)), device_id_type=MESH)

    @pl.loop(0, n_ep - 1 - e)
    def _(i):
        pl.semaphore_signal(barrier, inc=1, device_id=(at_rank(n_ep - 1 - i), t), device_id_type=MESH)

    loads(0).wait()
    loads(1).wait()
    stream = tok[...].astype(F32)
    scale = lax.rsqrt(jnp.mean(stream * stream, axis=-1, keepdims=True) + EPSILON)
    normed = (stream * scale * again[...].reshape(1, -1).astype(F32)).astype(BF)
    loads(3).wait()
    for i in (4, 5, 6, 7):
        loads(i).start()
    load_len.start()
    for row in range(HEADS):
        pltpu.make_async_copy(
            sources[11].at[0, pl.ds(2 * (row % n_tp) + row // n_tp, 1)],
            lc.at[0, pl.ds(row, 1)],
            in_sem.at[11],
        ).start()
    for i in (12, 13, 14, 9, 10, 8, 2, 15, 16, 17):
        loads(i).start()
    q_send[...] = dot(normed, wq[...]).astype(BF).astype(F32)
    pl.semaphore_wait(barrier, n_tp - 1 + e)

    def q_copy(i):
        to = tp_peer(i)
        return pltpu.make_async_remote_copy(
            src_ref=q_send.at[pl.ds(to, 1)], dst_ref=q_recv.at[pl.ds(t, 1)],
            send_sem=q_ss, recv_sem=q_rs, device_id=(ep, to), device_id_type=MESH,
        )

    @pl.loop(0, n_tp - 1, unroll=True)
    def _(i):
        q_copy(i).start()

    late_one = (e >= late).astype(jnp.int32)

    @pl.loop(0, e)
    def _(i):
        pl.semaphore_signal(
            ready.at[late_one], inc=1, device_id=(at_rank(i), t), device_id_type=MESH
        )

    own = iota((rows, 1), 0) == t
    for i in (4, 5, 6, 7):
        loads(i).wait()

    def own_row(value):
        return jnp.sum(jnp.where(own, value, 0.0), axis=0, keepdims=True)

    key_new = own_row(dot(normed, wk[...])).astype(BF).astype(F32)
    value_new = own_row(dot(normed, wv[...])).astype(BF).astype(F32)
    head = 2 * (iota((HEADS, 1), 0) % n_tp) + iota((HEADS, 1), 0) // n_tp
    head_lane = head == iota((HEADS, HEADS), 1)
    bias = jnp.sum(jnp.where(head_lane, fb[...].reshape(1, -1), 0.0), axis=1, keepdims=True)
    gate_all = dot_t(normed, wf[...])
    gate_in = jnp.sum(jnp.where(head_lane, own_row(gate_all), 0.0), axis=1, keepdims=True) + bias
    log_gate = jnp.minimum(gate_in, 0.0) - jnp.log1p(jnp.exp(-jnp.abs(gate_in)))
    loads(11).wait()
    load_len.wait()
    length = len_ref[0]
    logcum = lc[0]
    position = iota((1, logcum.shape[1]), 1)
    latest = jnp.sum(jnp.where(position == length - 1, logcum, 0.0), axis=1, keepdims=True)
    decay[...] = jnp.where(position < length, (latest + log_gate) - logcum, MASKED_SCORE)

    for i in (12, 13, 14):
        loads(i).wait()
    eye_rows = iota((rows, rows), 0) == iota((rows, rows), 1)

    def column(row, zero):
        return jnp.sum(jnp.where(eye_rows, row, zero), axis=1, keepdims=True)

    chosen = rg[...].reshape(1, -1) * (n_ep // GROUPS) + re[...]
    chosen = rank_of(chosen)
    slot_row = iota((picks, rows), 0)
    named = jnp.logical_or(
        chosen[0:1, :] == slot_row // SLOTS, chosen[1:2, :] == slot_row // SLOTS
    )
    named = named.astype(F32)
    before = (iota((rows, rows), 0) < iota((rows, rows), 1)).astype(F32).astype(BF)
    earlier = dot(named.astype(BF), before)
    place = jnp.where(earlier == (slot_row % SLOTS).astype(F32), named, 0.0).astype(BF)
    slot_lane = iota((rows, picks), 1)
    first = column(chosen[0:1, :], 0) == slot_lane // SLOTS
    second = column(chosen[1:2, :], 0) == slot_lane // SLOTS
    named_t = jnp.logical_or(first, second).astype(F32)
    before_t = (iota((rows, rows), 1) < iota((rows, rows), 0)).astype(F32).astype(BF)
    earlier_t = dot(before_t, named_t.astype(BF))
    here = earlier_t == (slot_lane % SLOTS).astype(F32)
    weight_t = jnp.where(first, column(rw[0:1, :], 0.0), column(rw[1:2, :], 0.0))
    combine = exact_parts(jnp.where(here, named_t * weight_t, 0.0))

    pltpu.make_async_copy(q_recv.at[pl.ds(0, n_tp - 1)], q_recv.at[pl.ds(0, n_tp - 1)], q_rs).wait()
    q16 = jnp.where(iota((n_tp, 1), 0) == t, q_send[...], q_recv[...]) * (HEAD ** (-0.5))
    turned = pltpu.roll(q16, HEAD, 1)
    low = iota((n_tp, 2 * HEAD), 1) < HEAD
    q_both = jnp.concatenate(
        [jnp.where(low, q16, turned), jnp.where(low, turned, q16)], axis=0
    )
    q_wide = jnp.concatenate([q_both] * (KV_HEADS // 2), axis=1)
    kv_width = KV_HEADS * HEAD
    mine = iota((HEADS, kv_width), 1) // HEAD == head // (HEADS // KV_HEADS)
    q_wide = jnp.where(mine, q_wide, 0.0)
    own_score = jnp.sum(q_wide * key_new, axis=1, keepdims=True)
    loads(9).wait()
    scores = dot_t(q_wide.astype(BF), ck[0]) + decay[...]
    peak = jnp.maximum(jnp.max(scores, axis=1, keepdims=True), own_score)
    weights = jnp.exp(scores - peak)
    own_weight = jnp.exp(own_score - peak)
    denominator = jnp.sum(weights, axis=1, keepdims=True) + own_weight
    loads(10).wait()
    summed = dot(weights.astype(BF), cv[0])
    summed = summed + own_weight.astype(BF).astype(F32) * value_new
    summed = jnp.where(mine, summed, 0.0)
    folded = summed[:, : 2 * HEAD]
    for k in range(1, KV_HEADS // 2):
        folded = folded + summed[:, k * 2 * HEAD : (k + 1) * 2 * HEAD]
    folded = (folded + pltpu.roll(folded, HEAD, 1)) / denominator
    att_all[t] = jnp.where(low, folded[:n_tp], folded[n_tp:]).astype(BF)

    def att_copy(i):
        return pltpu.make_async_remote_copy(
            src_ref=att_all.at[t], dst_ref=att_all.at[t],
            send_sem=a_ss, recv_sem=a_rs, device_id=(ep, tp_peer(i)), device_id_type=MESH,
        )

    @pl.loop(0, n_tp - 1, unroll=True)
    def _(i):
        att_copy(i).start()

    residual = tok[:, pl.ds(pl.multiple_of(t * width, width), width)].astype(F32)
    loads(8).wait()
    pltpu.make_async_copy(
        att_all.at[pl.ds(0, n_tp - 1)], att_all.at[pl.ds(0, n_tp - 1)], a_rs
    ).wait()
    att_rows[...] = att_all[...].reshape(n_tp * n_tp, 2 * HEAD).astype(F32)
    attended = jnp.concatenate(
        [att_rows[pl.ds(k, n_tp, stride=n_tp), :].astype(BF) for k in range(n_tp)], axis=1
    )
    mixed = (residual + dot(attended, wo[...])).astype(BF)

    d_send[...] = dot(place, mixed).astype(BF)

    def pick_copy(to, src, dst, ss, rs):
        return pltpu.make_async_remote_copy(
            src_ref=src.at[pl.ds(pl.multiple_of(to * SLOTS, SLOTS), SLOTS)],
            dst_ref=dst.at[pl.ds(pl.multiple_of(e * SLOTS, SLOTS), SLOTS)],
            send_sem=ss, recv_sem=rs, device_id=(at_rank(to), t), device_id_type=MESH,
        )

    def slots_wait(ref, sem, count):
        part = ref.at[pl.ds(0, count * SLOTS)]
        return pltpu.make_async_copy(part, part, sem).wait()

    batch = sum((e >= first).astype(jnp.int32) for first in bounds[1:-1])

    def send_picks(first, last):
        @pl.loop(first, last, unroll=True)
        def _(i):
            to = i + (i >= e).astype(jnp.int32)
            pick_copy(to, d_send, d_recv, d_ss, d_rs.at[batch]).start()

    @pl.when(e < late - 1)
    def _():
        pl.semaphore_wait(ready.at[0], late - 1 - e)

    send_picks(0, late - 1)

    @pl.when(e < n_ep - 1)
    def _():
        pl.semaphore_wait(ready.at[1], jnp.minimum(n_ep - late, n_ep - 1 - e))

    send_picks(late - 1, n_ep - 1)

    own_slots = iota((picks, 1), 0) // SLOTS == e
    far_first = sorted(range(1, n_y), key=lambda d: -min(d, n_y - d))
    partner = 2 * y + 1 - c

    def column_copy(buf, d, sems):
        to = 2 * lax.rem(y + d, n_y) + 1 - c
        return pltpu.make_async_remote_copy(
            src_ref=buf.at[t], dst_ref=buf.at[t], send_sem=sems[0].at[0],
            recv_sem=sems[1].at[d - 1], device_id=(ep, to), device_id_type=MESH,
        )

    def pass_on(buf, d, sems):
        slot = 2 * lax.rem(y + n_y - d, n_y) + (c if d == 0 else 1 - c)
        return pltpu.make_async_remote_copy(
            src_ref=buf.at[slot], dst_ref=buf.at[slot], send_sem=sems[0].at[1],
            recv_sem=sems[0].at[2], device_id=(ep, partner), device_id_type=MESH,
        )

    def wait_parts(buf, count, sem):
        part = buf.at[pl.ds(0, count)]
        pltpu.make_async_copy(part, part, sem).wait()

    def gather_start(buf, sems):
        for d in far_first:
            column_copy(buf, d, sems).start()
        pass_on(buf, 0, sems).start()

    def gather_pass(buf, sems):
        for d in far_first[::-1]:
            column_copy(buf, d, sems).wait_recv()
            pass_on(buf, d, sems).start()

    def gather_finish(buf, sems):
        wait_parts(buf, n_y, sems[0].at[2])

    def gather_end(buf, sems):
        wait_parts(buf, n_y - 1, sems[0].at[0])
        wait_parts(buf, n_y, sems[0].at[1])

    def arrive(k):
        count = bounds[k + 1] - bounds[k]
        slots = slice(bounds[k] * SLOTS, bounds[k + 1] * SLOTS)

        @pl.when(batch == k)
        def _():
            slots_wait(d_recv, d_rs.at[k], count - 1)

        @pl.when(batch != k)
        def _():
            slots_wait(d_recv, d_rs.at[k], count)

        x_all[k][t] = jnp.where(
            own_slots[slots], d_send[slots, :].astype(F32), d_recv[slots, :].astype(F32)
        ).astype(BF)
        gather_start(x_all[k], x_sems[k])

    def expand(k):
        gather_finish(x_all[k], x_sems[k])
        buf = x_all[k]
        total = jnp.zeros(buf.shape[1:], F32)
        for j in range(n_tp):
            part = buf[j].astype(F32)
            total = total + part * part
        scale = lax.rsqrt(jnp.sum(total, axis=1, keepdims=True) / (n_tp * width) + EPSILON)
        gain = fgain[...].reshape(1, -1).astype(F32)
        moe_in = jnp.concatenate(
            [
                (buf[j].astype(F32) * scale * gain[:, j * width : (j + 1) * width]).astype(BF)
                for j in range(n_tp)
            ],
            axis=1,
        )
        gated = dot(moe_in, wg[0])
        up = dot(moe_in, wu[0])
        h_all[k][t] = (gated / (1.0 + jnp.exp(-gated)) * up).astype(BF)
        gather_start(h_all[k], h_sems[k])

    def contract(k):
        slots = slice(bounds[k] * SLOTS, bounds[k + 1] * SLOTS)
        gather_finish(h_all[k], h_sems[k])
        hidden = jnp.concatenate([h_all[k][j] for j in range(n_tp)], axis=1)
        r_send[slots, :] = dot(hidden, wd[0]).astype(BF)

        @pl.loop(bounds[k], bounds[k + 1], unroll=True)
        def _(to):
            @pl.when(to != e)
            def _():
                pick_copy(to, r_send, r_recv, r_ss, r_rs).start()

    n_batches = len(bounds) - 1

    def work(order):
        passed = set()

        def once(kind, k):
            if (kind, k) not in passed:
                passed.add((kind, k))
                if kind == "x":
                    gather_pass(x_all[k], x_sems[k])
                else:
                    gather_pass(h_all[k], h_sems[k])

        for step in order.split():
            kind, k = step[0], int(step[1])
            if kind == "a":
                arrive(k)
            elif kind == "p":
                once("x", k)
            elif kind == "q":
                once("h", k)
            elif kind == "x":
                once("x", k)
                expand(k)
            else:
                once("h", k)
                contract(k)

    for i in (2, 15, 16, 17):
        loads(i).wait()
    for low, high, order in orders:
        @pl.when(jnp.logical_and(e >= low, e < high))
        def _(order=order):
            work(order)

    slots_wait(r_recv, r_rs, n_ep - 1)
    back = jnp.where(own_slots, r_send[...].astype(F32), r_recv[...].astype(F32)).astype(BF)
    moe_sum = sum(dot(part, back) for part in combine[::-1])
    out_ref[...] = mixed.astype(F32) + moe_sum

    pltpu.make_async_copy(q_send.at[pl.ds(0, n_tp - 1)], q_send.at[pl.ds(0, n_tp - 1)], q_ss).wait()
    pltpu.make_async_copy(
        att_all.at[pl.ds(0, n_tp - 1)], att_all.at[pl.ds(0, n_tp - 1)], a_ss
    ).wait()
    slots_wait(d_send, d_ss, n_ep - 1)
    for k in range(n_batches):
        gather_end(x_all[k], x_sems[k])
        gather_end(h_all[k], h_sems[k])
    slots_wait(r_send, r_ss, n_ep - 1)


def batch_bounds(n_ep):
    return (0, n_ep // 3, n_ep * 2 // 3, n_ep)


def plan_orders(n_ep):
    early, middle, late = n_ep // 3, n_ep // 2, n_ep * 2 // 3
    return (
        (0, early, "a0 x0 a1 a2 q0 p1 x1 p2 x2 h0 h1 h2"),
        (early, middle, "a0 x0 a1 a2 q0 p1 h0 x1 p2 x2 h1 h2"),
        (middle, late, "a0 a1 x0 a2 x1 h0 x2 h1 h2"),
        (late, n_ep, "a0 a1 a2 x0 x1 x2 h0 h1 h2"),
    )


def on_device(*args):
    args = list(args)
    for i in (6, 14, 15):
        args[i] = args[i].T
    n_ep = lax.axis_size("ep")
    n_tp = lax.axis_size("tp")
    rows = args[0].shape[0]
    width = args[8].shape[1]
    picks = n_ep * SLOTS
    bounds = batch_bounds(n_ep)
    sizes = [(b - a) * SLOTS for a, b in zip(bounds, bounds[1:])]
    any_spec = pl.BlockSpec(memory_space=pltpu.HBM)
    specs = [any_spec] * 19
    held = [pltpu.VMEM(a.shape, a.dtype) for i, a in enumerate(args) if i != 12]
    dma = pltpu.SemaphoreType.DMA
    scratch = held + [
        pltpu.VMEM((rows, width), F32),
        pltpu.VMEM((n_tp, width), F32),
        pltpu.VMEM((n_tp, n_tp, 2 * HEAD), BF),
        pltpu.VMEM((n_tp * n_tp, 2 * HEAD), F32),
        pltpu.VMEM((picks, width), BF),
        pltpu.VMEM((picks, width), BF),
        pltpu.VMEM((picks, width), BF),
        pltpu.VMEM((picks, width), BF),
        pltpu.VMEM(args[11].shape[1:], F32),
        pltpu.SMEM((1,), jnp.int32),
    ]
    scratch += [pltpu.VMEM((n_tp, size, width), BF) for size in sizes + sizes]
    scratch += [dma((18,)), dma, dma, dma, dma, dma, dma, dma((len(sizes),)), dma, dma]
    scratch += [pltpu.SemaphoreType.REGULAR((2,))]
    for _ in range(2):
        scratch += [dma((3,)) for _ in sizes] + [dma((n_tp // 2 - 1,)) for _ in sizes]
    args = [
        a if i == 12 else pltpu.with_memory_space_constraint(a, pltpu.HBM)
        for i, a in enumerate(args)
    ]
    return pl.pallas_call(
        functools.partial(layer_kernel, n_ep, n_tp, bounds, plan_orders(n_ep)),
        out_shape=jax.ShapeDtypeStruct((rows, width), F32),
        in_specs=specs,
        out_specs=pl.BlockSpec(memory_space=pltpu.VMEM),
        scratch_shapes=scratch,
        compiler_params=pltpu.CompilerParams(
            collective_id=0, has_side_effects=True, vmem_limit_bytes=24 * 1024 * 1024
        ),
        name="layer",
    )(*args).astype(BF)


def solution(mesh):
    placed = (
        P("ep", None),
        P(),
        P(),
        P(None, "tp"),
        P(),
        P(),
        P(),
        P(),
        P(None, "tp"),
        P(("ep", "tp"), None, None),
        P(("ep", "tp"), None, None),
        P(("ep", "tp"), None, None),
        P(("ep", "tp")),
        P("ep"),
        P("ep", None),
        P("ep", None),
        P("ep", None, "tp"),
        P("ep", None, "tp"),
        P("ep", None, "tp"),
    )
    return jax.shard_map(
        on_device, mesh=mesh, in_specs=placed, out_specs=P("ep", "tp"), check_vma=False
    )
```

```python
import functools

import jax
import jax.numpy as jnp
from jax import lax
from jax.experimental import pallas as pl
from jax.experimental.pallas import tpu as pltpu
from jax.sharding import PartitionSpec as P

HEADS = 32
KV_HEADS = 4
HEAD = 64
GROUPS = 4
EPSILON = 1e-06
MASKED_SCORE = -1e30
SLOTS = 2
BF = jnp.bfloat16
F32 = jnp.float32
MESH = pl.DeviceIdType.MESH


def iota(shape, dim):
    return lax.broadcasted_iota(jnp.int32, shape, dim)


def dot(a, b):
    return jnp.dot(a, b, preferred_element_type=F32)


def dot_t(a, b):
    return lax.dot_general(a, b, (((1,), (1,)), ((), ())), preferred_element_type=F32)


def exact_parts(x):
    a = x.astype(BF)
    r = x - a.astype(F32)
    b = r.astype(BF)
    return a, b, (r - b.astype(F32)).astype(BF)


def layer_kernel(n_ep, n_tp, bounds, orders, *refs):
    inputs, out_ref, rest = refs[:19], refs[19], refs[20:]
    held, scratch = rest[:18], rest[18:]
    (tok, again, fgain, wq, wk, wv, wf, fb, wo, ck, cv, lc, rg, re, rw, wg, wu, wd) = held
    sources = inputs[:12] + inputs[13:]
    count = len(bounds) - 1
    scratch = list(scratch)

    def take(number):
        taken = scratch[:number]
        del scratch[:number]
        return taken

    q_send, q_recv, att_all, att_rows, d_send, d_recv, r_send, r_recv, decay, keys_t, len_ref = take(11)
    x_all, h_all = take(count), take(count)
    in_sem, len_sem, q_ss, q_rs, a_ss, a_rs, d_ss, d_rs, r_ss, r_rs, ready = take(11)
    x_sems, h_sems = take(count), take(count)
    ep = lax.axis_index("ep")
    zero_rank = n_ep // 3 - 1

    def rank_of(place):
        return jnp.where(place == 0, zero_rank, place - (place <= zero_rank).astype(jnp.int32))

    e = rank_of(ep)
    t = lax.axis_index("tp")
    n_y = n_tp // 2
    y, c = t // 2, t % 2
    rows = tok.shape[0]
    late = n_ep * 2 // 3
    picks = n_ep * SLOTS
    width = wo.shape[1]

    def at_rank(rank):
        return jnp.where(rank == zero_rank, 0, rank + (rank < zero_rank).astype(jnp.int32))

    def tp_peer(i):
        k = (i + 1) // 2
        return lax.rem(t + n_tp // 2 + k * (1 - 2 * (i % 2)) + n_tp, n_tp)

    def loads(i):
        return pltpu.make_async_copy(sources[i], held[i], in_sem.at[i])

    for i in (0, 1, 3):
        loads(i).start()
    load_len = pltpu.make_async_copy(inputs[12], len_ref, len_sem)

    barrier = pltpu.get_barrier_semaphore()

    @pl.loop(0, n_tp - 1)
    def _(i):
        pl.semaphore_signal(barrier, inc=1, device_id=(ep, tp_peer(i)), device_id_type=MESH)

    @pl.loop(0, n_ep - 1 - e)
    def _(i):
        pl.semaphore_signal(barrier, inc=1, device_id=(at_rank(n_ep - 1 - i), t), device_id_type=MESH)

    loads(0).wait()
    loads(1).wait()
    stream = tok[...].astype(F32)
    scale = lax.rsqrt(jnp.mean(stream * stream, axis=-1, keepdims=True) + EPSILON)
    normed = (stream * scale * again[...].reshape(1, -1).astype(F32)).astype(BF)
    loads(3).wait()
    for i in (4, 5, 6, 7):
        loads(i).start()
    load_len.start()
    for row in range(HEADS):
        pltpu.make_async_copy(
            sources[11].at[0, pl.ds(2 * (row % n_tp) + row // n_tp, 1)],
            lc.at[0, pl.ds(row, 1)],
            in_sem.at[11],
        ).start()
    for i in (12, 13, 14, 9, 10, 8, 2, 15, 16, 17):
        loads(i).start()
    q_send[...] = dot(normed, wq[...]).astype(BF).astype(F32)
    pl.semaphore_wait(barrier, n_tp - 1 + e)

    def q_copy(i):
        to = tp_peer(i)
        return pltpu.make_async_remote_copy(
            src_ref=q_send.at[pl.ds(to, 1)], dst_ref=q_recv.at[pl.ds(t, 1)],
            send_sem=q_ss, recv_sem=q_rs, device_id=(ep, to), device_id_type=MESH,
        )

    @pl.loop(0, n_tp - 1, unroll=True)
    def _(i):
        q_copy(i).start()

    late_one = (e >= late).astype(jnp.int32)

    @pl.loop(0, e)
    def _(i):
        pl.semaphore_signal(
            ready.at[late_one], inc=1, device_id=(at_rank(i), t), device_id_type=MESH
        )

    own = iota((rows, 1), 0) == t
    for i in (4, 5, 6, 7):
        loads(i).wait()

    def own_row(value):
        return jnp.sum(jnp.where(own, value, 0.0), axis=0, keepdims=True)

    key_new = own_row(dot(normed, wk[...])).astype(BF).astype(F32)
    value_new = own_row(dot(normed, wv[...])).astype(BF).astype(F32)
    head = 2 * (iota((HEADS, 1), 0) % n_tp) + iota((HEADS, 1), 0) // n_tp
    head_lane = head == iota((HEADS, HEADS), 1)
    bias = jnp.sum(jnp.where(head_lane, fb[...].reshape(1, -1), 0.0), axis=1, keepdims=True)
    gate_all = dot_t(normed, wf[...])
    gate_in = jnp.sum(jnp.where(head_lane, own_row(gate_all), 0.0), axis=1, keepdims=True) + bias
    log_gate = jnp.minimum(gate_in, 0.0) - jnp.log1p(jnp.exp(-jnp.abs(gate_in)))
    loads(11).wait()
    load_len.wait()
    length = len_ref[0]
    logcum = lc[0]
    position = iota((1, logcum.shape[1]), 1)
    latest = jnp.sum(jnp.where(position == length - 1, logcum, 0.0), axis=1, keepdims=True)
    decay[...] = jnp.where(position < length, (latest + log_gate) - logcum, MASKED_SCORE)

    for i in (12, 13, 14):
        loads(i).wait()
    eye_rows = iota((rows, rows), 0) == iota((rows, rows), 1)

    def column(row, zero):
        return jnp.sum(jnp.where(eye_rows, row, zero), axis=1, keepdims=True)

    chosen = rg[...].reshape(1, -1) * (n_ep // GROUPS) + re[...]
    chosen = rank_of(chosen)
    slot_row = iota((picks, rows), 0)
    named = jnp.logical_or(
        chosen[0:1, :] == slot_row // SLOTS, chosen[1:2, :] == slot_row // SLOTS
    )
    named = named.astype(F32)
    before = (iota((rows, rows), 0) < iota((rows, rows), 1)).astype(F32).astype(BF)
    earlier = dot(named.astype(BF), before)
    place = jnp.where(earlier == (slot_row % SLOTS).astype(F32), named, 0.0).astype(BF)
    slot_lane = iota((rows, picks), 1)
    first = column(chosen[0:1, :], 0) == slot_lane // SLOTS
    second = column(chosen[1:2, :], 0) == slot_lane // SLOTS
    named_t = jnp.logical_or(first, second).astype(F32)
    before_t = (iota((rows, rows), 1) < iota((rows, rows), 0)).astype(F32).astype(BF)
    earlier_t = dot(before_t, named_t.astype(BF))
    here = earlier_t == (slot_lane % SLOTS).astype(F32)
    weight_t = jnp.where(first, column(rw[0:1, :], 0.0), column(rw[1:2, :], 0.0))
    combine = exact_parts(jnp.where(here, named_t * weight_t, 0.0))

    loads(9).wait()
    keys_t[...] = ck[0].T

    pltpu.make_async_copy(q_recv.at[pl.ds(0, n_tp - 1)], q_recv.at[pl.ds(0, n_tp - 1)], q_rs).wait()
    q16 = jnp.where(iota((n_tp, 1), 0) == t, q_send[...], q_recv[...]) * (HEAD ** (-0.5))
    turned = pltpu.roll(q16, HEAD, 1)
    low = iota((n_tp, 2 * HEAD), 1) < HEAD
    q_both = jnp.concatenate(
        [jnp.where(low, q16, turned), jnp.where(low, turned, q16)], axis=0
    )
    q_wide = jnp.concatenate([q_both] * (KV_HEADS // 2), axis=1)
    kv_width = KV_HEADS * HEAD
    mine = iota((HEADS, kv_width), 1) // HEAD == head // (HEADS // KV_HEADS)
    q_wide = jnp.where(mine, q_wide, 0.0)
    own_score = jnp.sum(q_wide * key_new, axis=1, keepdims=True)
    scores = dot(q_wide.astype(BF), keys_t[...]) + decay[...]
    peak = jnp.maximum(jnp.max(scores, axis=1, keepdims=True), own_score)
    weights = jnp.exp(scores - peak)
    own_weight = jnp.exp(own_score - peak)
    denominator = jnp.sum(weights, axis=1, keepdims=True) + own_weight
    loads(10).wait()
    summed = dot(weights.astype(BF), cv[0])
    summed = summed + own_weight.astype(BF).astype(F32) * value_new
    summed = jnp.where(mine, summed, 0.0)
    folded = summed[:, : 2 * HEAD]
    for k in range(1, KV_HEADS // 2):
        folded = folded + summed[:, k * 2 * HEAD : (k + 1) * 2 * HEAD]
    folded = (folded + pltpu.roll(folded, HEAD, 1)) / denominator
    att_all[t] = jnp.where(low, folded[:n_tp], folded[n_tp:]).astype(BF)

    def att_copy(i):
        return pltpu.make_async_remote_copy(
            src_ref=att_all.at[t], dst_ref=att_all.at[t],
            send_sem=a_ss, recv_sem=a_rs, device_id=(ep, tp_peer(i)), device_id_type=MESH,
        )

    @pl.loop(0, n_tp - 1, unroll=True)
    def _(i):
        att_copy(i).start()

    residual = tok[:, pl.ds(pl.multiple_of(t * width, width), width)].astype(F32)
    loads(8).wait()
    pltpu.make_async_copy(
        att_all.at[pl.ds(0, n_tp - 1)], att_all.at[pl.ds(0, n_tp - 1)], a_rs
    ).wait()
    att_rows[...] = att_all[...].reshape(n_tp * n_tp, 2 * HEAD).astype(F32)
    attended = jnp.concatenate(
        [att_rows[pl.ds(k, n_tp, stride=n_tp), :].astype(BF) for k in range(n_tp)], axis=1
    )
    mixed = (residual + dot(attended, wo[...])).astype(BF)

    d_send[...] = dot(place, mixed).astype(BF)

    def pick_copy(to, src, dst, ss, rs):
        return pltpu.make_async_remote_copy(
            src_ref=src.at[pl.ds(pl.multiple_of(to * SLOTS, SLOTS), SLOTS)],
            dst_ref=dst.at[pl.ds(pl.multiple_of(e * SLOTS, SLOTS), SLOTS)],
            send_sem=ss, recv_sem=rs, device_id=(at_rank(to), t), device_id_type=MESH,
        )

    def slots_wait(ref, sem, count):
        part = ref.at[pl.ds(0, count * SLOTS)]
        return pltpu.make_async_copy(part, part, sem).wait()

    batch = sum((e >= first).astype(jnp.int32) for first in bounds[1:-1])

    def send_picks(first, last):
        @pl.loop(first, last, unroll=True)
        def _(i):
            to = i + (i >= e).astype(jnp.int32)
            pick_copy(to, d_send, d_recv, d_ss, d_rs.at[batch]).start()

    @pl.when(e < late - 1)
    def _():
        pl.semaphore_wait(ready.at[0], late - 1 - e)

    send_picks(0, late - 1)

    @pl.when(e < n_ep - 1)
    def _():
        pl.semaphore_wait(ready.at[1], jnp.minimum(n_ep - late, n_ep - 1 - e))

    send_picks(late - 1, n_ep - 1)

    own_slots = iota((picks, 1), 0) // SLOTS == e
    far_first = sorted(range(1, n_y), key=lambda d: -min(d, n_y - d))
    partner = 2 * y + 1 - c

    def column_copy(buf, d, sems):
        to = 2 * lax.rem(y + d, n_y) + 1 - c
        return pltpu.make_async_remote_copy(
            src_ref=buf.at[t], dst_ref=buf.at[t], send_sem=sems.at[0],
            recv_sem=sems.at[1 + min(d, n_y - d)], device_id=(ep, to), device_id_type=MESH,
        )

    def pass_on(buf, d, sems):
        slot = 2 * lax.rem(y + n_y - d, n_y) + (c if d == 0 else 1 - c)
        return pltpu.make_async_remote_copy(
            src_ref=buf.at[slot], dst_ref=buf.at[slot], send_sem=sems.at[0],
            recv_sem=sems.at[1], device_id=(ep, partner), device_id_type=MESH,
        )

    def wait_parts(buf, count, sem):
        part = buf.at[pl.ds(0, count)]
        pltpu.make_async_copy(part, part, sem).wait()

    def gather_start(buf, sems):
        for d in far_first:
            column_copy(buf, d, sems).start()
        pass_on(buf, 0, sems).start()

    def gather_pass(buf, sems):
        for d in range(1, n_y // 2 + 1):
            both = sorted({d, n_y - d})
            wait_parts(buf, len(both), sems.at[1 + d])
            for side in both:
                pass_on(buf, side, sems).start()

    def gather_finish(buf, sems):
        wait_parts(buf, n_y, sems.at[1])

    def gather_end(buf, sems):
        wait_parts(buf, 2 * n_y - 1, sems.at[0])

    def arrive(k):
        count = bounds[k + 1] - bounds[k]
        slots = slice(bounds[k] * SLOTS, bounds[k + 1] * SLOTS)

        @pl.when(batch == k)
        def _():
            slots_wait(d_recv, d_rs.at[k], count - 1)

        @pl.when(batch != k)
        def _():
            slots_wait(d_recv, d_rs.at[k], count)

        x_all[k][t] = jnp.where(
            own_slots[slots], d_send[slots, :].astype(F32), d_recv[slots, :].astype(F32)
        ).astype(BF)
        gather_start(x_all[k], x_sems[k])

    def expand(k):
        gather_finish(x_all[k], x_sems[k])
        buf = x_all[k]
        total = jnp.zeros(buf.shape[1:], F32)
        for j in range(n_tp):
            part = buf[j].astype(F32)
            total = total + part * part
        scale = lax.rsqrt(jnp.sum(total, axis=1, keepdims=True) / (n_tp * width) + EPSILON)
        gain = fgain[...].reshape(1, -1).astype(F32)
        moe_in = jnp.concatenate(
            [
                (buf[j].astype(F32) * scale * gain[:, j * width : (j + 1) * width]).astype(BF)
                for j in range(n_tp)
            ],
            axis=1,
        )
        gated = dot(moe_in, wg[0])
        up = dot(moe_in, wu[0])
        h_all[k][t] = (gated / (1.0 + jnp.exp(-gated)) * up).astype(BF)
        gather_start(h_all[k], h_sems[k])

    def contract(k):
        slots = slice(bounds[k] * SLOTS, bounds[k + 1] * SLOTS)
        gather_finish(h_all[k], h_sems[k])
        hidden = jnp.concatenate([h_all[k][j] for j in range(n_tp)], axis=1)
        r_send[slots, :] = dot(hidden, wd[0]).astype(BF)

        @pl.loop(bounds[k], bounds[k + 1], unroll=True)
        def _(to):
            @pl.when(to != e)
            def _():
                pick_copy(to, r_send, r_recv, r_ss, r_rs).start()

    n_batches = len(bounds) - 1

    def work(order):
        passed = set()

        def once(kind, k):
            if (kind, k) not in passed:
                passed.add((kind, k))
                if kind == "x":
                    gather_pass(x_all[k], x_sems[k])
                else:
                    gather_pass(h_all[k], h_sems[k])

        for step in order.split():
            kind, k = step[0], int(step[1])
            if kind == "a":
                arrive(k)
            elif kind == "p":
                once("x", k)
            elif kind == "q":
                once("h", k)
            elif kind == "x":
                once("x", k)
                expand(k)
            else:
                once("h", k)
                contract(k)

    for i in (2, 15, 16, 17):
        loads(i).wait()
    for low, high, order in orders:
        @pl.when(jnp.logical_and(e >= low, e < high))
        def _(order=order):
            work(order)

    slots_wait(r_recv, r_rs, n_ep - 1)
    back = jnp.where(own_slots, r_send[...].astype(F32), r_recv[...].astype(F32)).astype(BF)
    moe_sum = sum(dot(part, back) for part in combine[::-1])
    out_ref[...] = mixed.astype(F32) + moe_sum

    pltpu.make_async_copy(q_send.at[pl.ds(0, n_tp - 1)], q_send.at[pl.ds(0, n_tp - 1)], q_ss).wait()
    pltpu.make_async_copy(
        att_all.at[pl.ds(0, n_tp - 1)], att_all.at[pl.ds(0, n_tp - 1)], a_ss
    ).wait()
    slots_wait(d_send, d_ss, n_ep - 1)
    for k in range(n_batches):
        gather_end(x_all[k], x_sems[k])
        gather_end(h_all[k], h_sems[k])
    slots_wait(r_send, r_ss, n_ep - 1)


def batch_bounds(n_ep):
    return (0, n_ep // 3, n_ep // 2, n_ep)


def plan_orders(n_ep):
    early, middle, late = n_ep // 3, n_ep // 2, n_ep * 2 // 3
    return (
        (0, early, "a0 x0 a1 a2 q0 p1 x1 p2 x2 h0 h1 h2"),
        (early, middle, "a0 x0 a1 a2 q0 p1 h0 x1 p2 x2 h1 h2"),
        (middle, late, "a0 a1 x0 a2 x1 h0 x2 h1 h2"),
        (late, n_ep, "a0 a1 a2 x0 x1 x2 h0 h1 h2"),
    )


def on_device(*args):
    args = list(args)
    for i in (6, 14, 15):
        args[i] = args[i].T
    n_ep = lax.axis_size("ep")
    n_tp = lax.axis_size("tp")
    rows = args[0].shape[0]
    width = args[8].shape[1]
    picks = n_ep * SLOTS
    bounds = batch_bounds(n_ep)
    sizes = [(b - a) * SLOTS for a, b in zip(bounds, bounds[1:])]
    any_spec = pl.BlockSpec(memory_space=pltpu.HBM)
    specs = [any_spec] * 19
    held = [pltpu.VMEM(a.shape, a.dtype) for i, a in enumerate(args) if i != 12]
    dma = pltpu.SemaphoreType.DMA
    scratch = held + [
        pltpu.VMEM((rows, width), F32),
        pltpu.VMEM((n_tp, width), F32),
        pltpu.VMEM((n_tp, n_tp, 2 * HEAD), BF),
        pltpu.VMEM((n_tp * n_tp, 2 * HEAD), F32),
        pltpu.VMEM((picks, width), BF),
        pltpu.VMEM((picks, width), BF),
        pltpu.VMEM((picks, width), BF),
        pltpu.VMEM((picks, width), BF),
        pltpu.VMEM(args[11].shape[1:], F32),
        pltpu.VMEM(args[9].shape[:0:-1], BF),
        pltpu.SMEM((1,), jnp.int32),
    ]
    scratch += [pltpu.VMEM((n_tp, size, width), BF) for size in sizes + sizes]
    scratch += [dma((18,)), dma, dma, dma, dma, dma, dma, dma((len(sizes),)), dma, dma]
    scratch += [pltpu.SemaphoreType.REGULAR((2,))]
    scratch += [dma((2 + n_tp // 4,)) for _ in sizes + sizes]
    args = [
        a if i == 12 else pltpu.with_memory_space_constraint(a, pltpu.HBM)
        for i, a in enumerate(args)
    ]
    return pl.pallas_call(
        functools.partial(layer_kernel, n_ep, n_tp, bounds, plan_orders(n_ep)),
        out_shape=jax.ShapeDtypeStruct((rows, width), F32),
        in_specs=specs,
        out_specs=pl.BlockSpec(memory_space=pltpu.VMEM),
        scratch_shapes=scratch,
        compiler_params=pltpu.CompilerParams(
            collective_id=0, has_side_effects=True, vmem_limit_bytes=24 * 1024 * 1024
        ),
        name="layer",
    )(*args).astype(BF)


def solution(mesh):
    placed = (
        P("ep", None),
        P(),
        P(),
        P(None, "tp"),
        P(),
        P(),
        P(),
        P(),
        P(None, "tp"),
        P(("ep", "tp"), None, None),
        P(("ep", "tp"), None, None),
        P(("ep", "tp"), None, None),
        P(("ep", "tp")),
        P("ep"),
        P("ep", None),
        P("ep", None),
        P("ep", None, "tp"),
        P("ep", None, "tp"),
        P("ep", None, "tp"),
    )
    return jax.shard_map(
        on_device, mesh=mesh, in_specs=placed, out_specs=P("ep", "tp"), check_vma=False
    )
```

```python
import functools

import jax
import jax.numpy as jnp
from jax import lax
from jax.experimental import pallas as pl
from jax.experimental.pallas import tpu as pltpu
from jax.sharding import PartitionSpec as P

HEADS = 32
KV_HEADS = 4
HEAD = 64
GROUPS = 4
EPSILON = 1e-06
MASKED_SCORE = -1e30
SLOTS = 2
BF = jnp.bfloat16
F32 = jnp.float32
MESH = pl.DeviceIdType.MESH


def iota(shape, dim):
    return lax.broadcasted_iota(jnp.int32, shape, dim)


def dot(a, b):
    return jnp.dot(a, b, preferred_element_type=F32)


def dot_t(a, b):
    return lax.dot_general(a, b, (((1,), (1,)), ((), ())), preferred_element_type=F32)


def exact_parts(x):
    a = x.astype(BF)
    r = x - a.astype(F32)
    b = r.astype(BF)
    return a, b, (r - b.astype(F32)).astype(BF)


def layer_kernel(n_ep, n_tp, bounds, orders, *refs):
    inputs, out_ref, rest = refs[:19], refs[19], refs[20:]
    held, scratch = rest[:18], rest[18:]
    (tok, again, fgain, wq, wk, wv, wf, fb, wo, ck, cv, lc, rg, re, rw, wg, wu, wd) = held
    sources = inputs[:12] + inputs[13:]
    count = len(bounds) - 1
    scratch = list(scratch)

    def take(number):
        taken = scratch[:number]
        del scratch[:number]
        return taken

    q_send, q_recv, att_all, att_rows, d_send, d_recv, r_send, r_recv, decay, keys_t, len_ref = take(11)
    x_all, h_all = take(count), take(count)
    in_sem, len_sem, q_ss, q_rs, a_ss, a_rs, d_ss, d_rs, r_ss, r_rs, ready = take(11)
    x_sems, h_sems = take(count), take(count)
    ep = lax.axis_index("ep")
    zero_rank = n_ep // 3 - 1

    def rank_of(place):
        return jnp.where(place == 0, zero_rank, place - (place <= zero_rank).astype(jnp.int32))

    e = rank_of(ep)
    t = lax.axis_index("tp")
    n_y = n_tp // 2
    y, c = t // 2, t % 2
    rows = tok.shape[0]
    late = n_ep * 2 // 3
    picks = n_ep * SLOTS
    width = wo.shape[1]

    def at_rank(rank):
        return jnp.where(rank == zero_rank, 0, rank + (rank < zero_rank).astype(jnp.int32))

    def tp_peer(i):
        k = (i + 1) // 2
        return lax.rem(t + n_tp // 2 + k * (1 - 2 * (i % 2)) + n_tp, n_tp)

    def loads(i):
        return pltpu.make_async_copy(sources[i], held[i], in_sem.at[i])

    for i in (0, 1, 3):
        loads(i).start()
    load_len = pltpu.make_async_copy(inputs[12], len_ref, len_sem)

    barrier = pltpu.get_barrier_semaphore()

    @pl.loop(0, n_tp - 1)
    def _(i):
        pl.semaphore_signal(barrier, inc=1, device_id=(ep, tp_peer(i)), device_id_type=MESH)

    @pl.loop(0, n_ep - 1 - e)
    def _(i):
        pl.semaphore_signal(barrier, inc=1, device_id=(at_rank(n_ep - 1 - i), t), device_id_type=MESH)

    loads(0).wait()
    loads(1).wait()
    stream = tok[...].astype(F32)
    scale = lax.rsqrt(jnp.mean(stream * stream, axis=-1, keepdims=True) + EPSILON)
    normed = (stream * scale * again[...].reshape(1, -1).astype(F32)).astype(BF)
    loads(3).wait()
    for i in (4, 5, 6, 7):
        loads(i).start()
    load_len.start()
    for row in range(HEADS):
        pltpu.make_async_copy(
            sources[11].at[0, pl.ds(2 * (row % n_tp) + row // n_tp, 1)],
            lc.at[0, pl.ds(row, 1)],
            in_sem.at[11],
        ).start()
    for i in (12, 13, 14, 9, 10, 8, 2, 15, 16, 17):
        loads(i).start()
    q_send[...] = dot(normed, wq[...]).astype(BF).astype(F32)
    pl.semaphore_wait(barrier, n_tp - 1 + e)

    def q_copy(i):
        to = tp_peer(i)
        return pltpu.make_async_remote_copy(
            src_ref=q_send.at[pl.ds(to, 1)], dst_ref=q_recv.at[pl.ds(t, 1)],
            send_sem=q_ss, recv_sem=q_rs, device_id=(ep, to), device_id_type=MESH,
        )

    @pl.loop(0, n_tp - 1, unroll=True)
    def _(i):
        q_copy(i).start()

    late_one = (e >= late).astype(jnp.int32)

    @pl.loop(0, e)
    def _(i):
        pl.semaphore_signal(
            ready.at[late_one], inc=1, device_id=(at_rank(i), t), device_id_type=MESH
        )

    own = iota((rows, 1), 0) == t
    for i in (4, 5, 6, 7):
        loads(i).wait()

    def own_row(value):
        return jnp.sum(jnp.where(own, value, 0.0), axis=0, keepdims=True)

    key_new = own_row(dot(normed, wk[...])).astype(BF).astype(F32)
    value_new = own_row(dot(normed, wv[...])).astype(BF).astype(F32)
    head = 2 * (iota((HEADS, 1), 0) % n_tp) + iota((HEADS, 1), 0) // n_tp
    head_lane = head == iota((HEADS, HEADS), 1)
    bias = jnp.sum(jnp.where(head_lane, fb[...].reshape(1, -1), 0.0), axis=1, keepdims=True)
    gate_all = dot_t(normed, wf[...])
    gate_in = jnp.sum(jnp.where(head_lane, own_row(gate_all), 0.0), axis=1, keepdims=True) + bias
    log_gate = jnp.minimum(gate_in, 0.0) - jnp.log1p(jnp.exp(-jnp.abs(gate_in)))
    loads(11).wait()
    load_len.wait()
    length = len_ref[0]
    logcum = lc[0]
    position = iota((1, logcum.shape[1]), 1)
    latest = jnp.sum(jnp.where(position == length - 1, logcum, 0.0), axis=1, keepdims=True)
    decay[...] = jnp.where(position < length, (latest + log_gate) - logcum, MASKED_SCORE)

    for i in (12, 13, 14):
        loads(i).wait()
    eye_rows = iota((rows, rows), 0) == iota((rows, rows), 1)

    def column(row, zero):
        return jnp.sum(jnp.where(eye_rows, row, zero), axis=1, keepdims=True)

    chosen = rg[...].reshape(1, -1) * (n_ep // GROUPS) + re[...]
    chosen = rank_of(chosen)
    slot_row = iota((picks, rows), 0)
    named = jnp.logical_or(
        chosen[0:1, :] == slot_row // SLOTS, chosen[1:2, :] == slot_row // SLOTS
    )
    named = named.astype(F32)
    before = (iota((rows, rows), 0) < iota((rows, rows), 1)).astype(F32).astype(BF)
    earlier = dot(named.astype(BF), before)
    place = jnp.where(earlier == (slot_row % SLOTS).astype(F32), named, 0.0).astype(BF)
    slot_lane = iota((rows, picks), 1)
    first = column(chosen[0:1, :], 0) == slot_lane // SLOTS
    second = column(chosen[1:2, :], 0) == slot_lane // SLOTS
    named_t = jnp.logical_or(first, second).astype(F32)
    before_t = (iota((rows, rows), 1) < iota((rows, rows), 0)).astype(F32).astype(BF)
    earlier_t = dot(before_t, named_t.astype(BF))
    here = earlier_t == (slot_lane % SLOTS).astype(F32)
    weight_t = jnp.where(first, column(rw[0:1, :], 0.0), column(rw[1:2, :], 0.0))
    combine = exact_parts(jnp.where(here, named_t * weight_t, 0.0))

    loads(9).wait()
    keys_t[...] = ck[0].T

    pltpu.make_async_copy(q_recv.at[pl.ds(0, n_tp - 1)], q_recv.at[pl.ds(0, n_tp - 1)], q_rs).wait()
    q16 = jnp.where(iota((n_tp, 1), 0) == t, q_send[...], q_recv[...]) * (HEAD ** (-0.5))
    turned = pltpu.roll(q16, HEAD, 1)
    low = iota((n_tp, 2 * HEAD), 1) < HEAD
    q_both = jnp.concatenate(
        [jnp.where(low, q16, turned), jnp.where(low, turned, q16)], axis=0
    )
    q_wide = jnp.concatenate([q_both] * (KV_HEADS // 2), axis=1)
    kv_width = KV_HEADS * HEAD
    mine = iota((HEADS, kv_width), 1) // HEAD == head // (HEADS // KV_HEADS)
    q_wide = jnp.where(mine, q_wide, 0.0)
    own_score = jnp.sum(q_wide * key_new, axis=1, keepdims=True)
    scores = dot(q_wide.astype(BF), keys_t[...]) + decay[...]
    peak = jnp.maximum(jnp.max(scores, axis=1, keepdims=True), own_score)
    weights = jnp.exp(scores - peak)
    own_weight = jnp.exp(own_score - peak)
    denominator = jnp.sum(weights, axis=1, keepdims=True) + own_weight
    loads(10).wait()
    summed = dot(weights.astype(BF), cv[0])
    summed = summed + own_weight.astype(BF).astype(F32) * value_new
    summed = jnp.where(mine, summed, 0.0)
    folded = summed[:, : 2 * HEAD]
    for k in range(1, KV_HEADS // 2):
        folded = folded + summed[:, k * 2 * HEAD : (k + 1) * 2 * HEAD]
    folded = (folded + pltpu.roll(folded, HEAD, 1)) / denominator
    att_all[t] = jnp.where(low, folded[:n_tp], folded[n_tp:]).astype(BF)

    def att_copy(i):
        return pltpu.make_async_remote_copy(
            src_ref=att_all.at[t], dst_ref=att_all.at[t],
            send_sem=a_ss, recv_sem=a_rs, device_id=(ep, tp_peer(i)), device_id_type=MESH,
        )

    @pl.loop(0, n_tp - 1, unroll=True)
    def _(i):
        att_copy(i).start()

    residual = tok[:, pl.ds(pl.multiple_of(t * width, width), width)].astype(F32)
    loads(8).wait()
    pltpu.make_async_copy(
        att_all.at[pl.ds(0, n_tp - 1)], att_all.at[pl.ds(0, n_tp - 1)], a_rs
    ).wait()
    att_rows[...] = att_all[...].reshape(n_tp * n_tp, 2 * HEAD).astype(F32)
    attended = jnp.concatenate(
        [att_rows[pl.ds(k, n_tp, stride=n_tp), :].astype(BF) for k in range(n_tp)], axis=1
    )
    mixed = (residual + dot(attended, wo[...])).astype(BF)

    d_send[...] = dot(place, mixed).astype(BF)

    def pick_copy(to, src, dst, ss, rs):
        return pltpu.make_async_remote_copy(
            src_ref=src.at[pl.ds(pl.multiple_of(to * SLOTS, SLOTS), SLOTS)],
            dst_ref=dst.at[pl.ds(pl.multiple_of(e * SLOTS, SLOTS), SLOTS)],
            send_sem=ss, recv_sem=rs, device_id=(at_rank(to), t), device_id_type=MESH,
        )

    def slots_wait(ref, sem, count):
        part = ref.at[pl.ds(0, count * SLOTS)]
        return pltpu.make_async_copy(part, part, sem).wait()

    batch = sum((e >= first).astype(jnp.int32) for first in bounds[1:-1])

    def send_picks(first, last):
        @pl.loop(first, last, unroll=True)
        def _(i):
            to = i + (i >= e).astype(jnp.int32)
            pick_copy(to, d_send, d_recv, d_ss, d_rs.at[batch]).start()

    @pl.when(e < late - 1)
    def _():
        pl.semaphore_wait(ready.at[0], late - 1 - e)

    send_picks(0, late - 1)

    @pl.when(e < n_ep - 1)
    def _():
        pl.semaphore_wait(ready.at[1], jnp.minimum(n_ep - late, n_ep - 1 - e))

    send_picks(late - 1, n_ep - 1)

    own_slots = iota((picks, 1), 0) // SLOTS == e
    far_first = sorted(range(1, n_y), key=lambda d: -min(d, n_y - d))
    partner = 2 * y + 1 - c

    def column_copy(buf, d, sems):
        to = 2 * lax.rem(y + d, n_y) + 1 - c
        return pltpu.make_async_remote_copy(
            src_ref=buf.at[t], dst_ref=buf.at[t], send_sem=sems.at[0],
            recv_sem=sems.at[1 + min(d, n_y - d)], device_id=(ep, to), device_id_type=MESH,
        )

    def pass_on(buf, d, sems):
        slot = 2 * lax.rem(y + n_y - d, n_y) + (c if d == 0 else 1 - c)
        return pltpu.make_async_remote_copy(
            src_ref=buf.at[slot], dst_ref=buf.at[slot], send_sem=sems.at[0],
            recv_sem=sems.at[1], device_id=(ep, partner), device_id_type=MESH,
        )

    def wait_parts(buf, count, sem):
        part = buf.at[pl.ds(0, count)]
        pltpu.make_async_copy(part, part, sem).wait()

    def gather_start(buf, sems):
        for d in far_first:
            column_copy(buf, d, sems).start()
        pass_on(buf, 0, sems).start()

    def gather_pass(buf, sems):
        for d in range(1, n_y // 2 + 1):
            both = sorted({d, n_y - d})
            wait_parts(buf, len(both), sems.at[1 + d])
            for side in both:
                pass_on(buf, side, sems).start()

    def gather_finish(buf, sems):
        wait_parts(buf, n_y, sems.at[1])

    def gather_end(buf, sems):
        wait_parts(buf, 2 * n_y - 1, sems.at[0])

    def arrive(k):
        count = bounds[k + 1] - bounds[k]
        slots = slice(bounds[k] * SLOTS, bounds[k + 1] * SLOTS)

        @pl.when(batch == k)
        def _():
            slots_wait(d_recv, d_rs.at[k], count - 1)

        @pl.when(batch != k)
        def _():
            slots_wait(d_recv, d_rs.at[k], count)

        x_all[k][t] = jnp.where(
            own_slots[slots], d_send[slots, :].astype(F32), d_recv[slots, :].astype(F32)
        ).astype(BF)
        gather_start(x_all[k], x_sems[k])

    def expand(k):
        gather_finish(x_all[k], x_sems[k])
        buf = x_all[k]
        total = jnp.zeros(buf.shape[1:], F32)
        for j in range(n_tp):
            part = buf[j].astype(F32)
            total = total + part * part
        scale = lax.rsqrt(jnp.sum(total, axis=1, keepdims=True) / (n_tp * width) + EPSILON)
        gain = fgain[...].reshape(1, -1).astype(F32)
        moe_in = jnp.concatenate(
            [
                (buf[j].astype(F32) * scale * gain[:, j * width : (j + 1) * width]).astype(BF)
                for j in range(n_tp)
            ],
            axis=1,
        )
        gated = dot(moe_in, wg[0])
        up = dot(moe_in, wu[0])
        h_all[k][t] = (gated / (1.0 + jnp.exp(-gated)) * up).astype(BF)
        gather_start(h_all[k], h_sems[k])

    def contract(k):
        slots = slice(bounds[k] * SLOTS, bounds[k + 1] * SLOTS)
        gather_finish(h_all[k], h_sems[k])
        hidden = jnp.concatenate([h_all[k][j] for j in range(n_tp)], axis=1)
        r_send[slots, :] = dot(hidden, wd[0]).astype(BF)

        @pl.loop(bounds[k], bounds[k + 1], unroll=True)
        def _(to):
            @pl.when(to != e)
            def _():
                pick_copy(to, r_send, r_recv, r_ss, r_rs).start()

    n_batches = len(bounds) - 1

    def work(order):
        passed = set()

        def once(kind, k):
            if (kind, k) not in passed:
                passed.add((kind, k))
                if kind == "x":
                    gather_pass(x_all[k], x_sems[k])
                else:
                    gather_pass(h_all[k], h_sems[k])

        for step in order.split():
            kind, k = step[0], int(step[1])
            if kind == "a":
                arrive(k)
            elif kind == "p":
                once("x", k)
            elif kind == "q":
                once("h", k)
            elif kind == "x":
                once("x", k)
                expand(k)
            else:
                once("h", k)
                contract(k)

    for i in (2, 15, 16, 17):
        loads(i).wait()
    for low, high, order in orders:
        @pl.when(jnp.logical_and(e >= low, e < high))
        def _(order=order):
            work(order)

    slots_wait(r_recv, r_rs, n_ep - 1)
    back = jnp.where(own_slots, r_send[...].astype(F32), r_recv[...].astype(F32)).astype(BF)
    moe_sum = sum(dot(part, back) for part in combine[::-1])
    out_ref[...] = mixed.astype(F32) + moe_sum

    pltpu.make_async_copy(q_send.at[pl.ds(0, n_tp - 1)], q_send.at[pl.ds(0, n_tp - 1)], q_ss).wait()
    pltpu.make_async_copy(
        att_all.at[pl.ds(0, n_tp - 1)], att_all.at[pl.ds(0, n_tp - 1)], a_ss
    ).wait()
    slots_wait(d_send, d_ss, n_ep - 1)
    for k in range(n_batches):
        gather_end(x_all[k], x_sems[k])
        gather_end(h_all[k], h_sems[k])
    slots_wait(r_send, r_ss, n_ep - 1)


def batch_bounds(n_ep):
    return (0, n_ep // 3, n_ep // 2, n_ep)


def plan_orders(n_ep):
    early, middle, late = n_ep // 3, n_ep // 2, n_ep * 2 // 3
    return (
        (0, early, "a0 x0 a1 a2 q0 p1 p2 h0 x1 x2 q1 q2 h1 h2"),
        (early, middle, "a0 x0 a1 a2 q0 p1 h0 x1 p2 x2 h1 h2"),
        (middle, late, "a0 a1 x0 a2 x1 h0 x2 h1 h2"),
        (late, n_ep, "a0 a1 a2 x0 x1 x2 h0 h1 h2"),
    )


def on_device(*args):
    args = list(args)
    for i in (6, 14, 15):
        args[i] = args[i].T
    n_ep = lax.axis_size("ep")
    n_tp = lax.axis_size("tp")
    rows = args[0].shape[0]
    width = args[8].shape[1]
    picks = n_ep * SLOTS
    bounds = batch_bounds(n_ep)
    sizes = [(b - a) * SLOTS for a, b in zip(bounds, bounds[1:])]
    any_spec = pl.BlockSpec(memory_space=pltpu.HBM)
    specs = [any_spec] * 19
    held = [pltpu.VMEM(a.shape, a.dtype) for i, a in enumerate(args) if i != 12]
    dma = pltpu.SemaphoreType.DMA
    scratch = held + [
        pltpu.VMEM((rows, width), F32),
        pltpu.VMEM((n_tp, width), F32),
        pltpu.VMEM((n_tp, n_tp, 2 * HEAD), BF),
        pltpu.VMEM((n_tp * n_tp, 2 * HEAD), F32),
        pltpu.VMEM((picks, width), BF),
        pltpu.VMEM((picks, width), BF),
        pltpu.VMEM((picks, width), BF),
        pltpu.VMEM((picks, width), BF),
        pltpu.VMEM(args[11].shape[1:], F32),
        pltpu.VMEM(args[9].shape[:0:-1], BF),
        pltpu.SMEM((1,), jnp.int32),
    ]
    scratch += [pltpu.VMEM((n_tp, size, width), BF) for size in sizes + sizes]
    scratch += [dma((18,)), dma, dma, dma, dma, dma, dma, dma((len(sizes),)), dma, dma]
    scratch += [pltpu.SemaphoreType.REGULAR((2,))]
    scratch += [dma((2 + n_tp // 4,)) for _ in sizes + sizes]
    args = [
        a if i == 12 else pltpu.with_memory_space_constraint(a, pltpu.HBM)
        for i, a in enumerate(args)
    ]
    return pl.pallas_call(
        functools.partial(layer_kernel, n_ep, n_tp, bounds, plan_orders(n_ep)),
        out_shape=jax.ShapeDtypeStruct((rows, width), F32),
        in_specs=specs,
        out_specs=pl.BlockSpec(memory_space=pltpu.VMEM),
        scratch_shapes=scratch,
        compiler_params=pltpu.CompilerParams(
            collective_id=0, has_side_effects=True, vmem_limit_bytes=24 * 1024 * 1024
        ),
        name="layer",
    )(*args).astype(BF)


def solution(mesh):
    placed = (
        P("ep", None),
        P(),
        P(),
        P(None, "tp"),
        P(),
        P(),
        P(),
        P(),
        P(None, "tp"),
        P(("ep", "tp"), None, None),
        P(("ep", "tp"), None, None),
        P(("ep", "tp"), None, None),
        P(("ep", "tp")),
        P("ep"),
        P("ep", None),
        P("ep", None),
        P("ep", None, "tp"),
        P("ep", None, "tp"),
        P("ep", None, "tp"),
    )
    return jax.shard_map(
        on_device, mesh=mesh, in_specs=placed, out_specs=P("ep", "tp"), check_vma=False
    )
```
